32 devices in a mesh: ep: 8 (over z, x), tp: 4 (over y, core).
Axes of the slice: x: 2, y: 2, z: 4, core: 2. Of those that a mesh axis runs over, the one named last changes fastest.
Arguments:
- tokens: bfloat16 [1024, 4096], P('ep', 'tp'), may hold values from -6 to 6
- cotangent: bfloat16 [1024, 4096], P('ep', 'tp'), may hold values from -6 to 6
- routes: int32 [1024, 2], P('ep'), may hold values from 0 to 7, all different within a row; in each aligned block of 128 rows (0 to 127, 128 to 255, ...) at most 48 rows name the same one
- gate_weight: float32 [1024, 2], P('ep'), may hold values from 0.1 to 2.5
- w_gate: bfloat16 [8, 1024, 4096], P('ep', 'tp'), may hold values from -0.09375 to 0.09375
- w_up: bfloat16 [8, 1024, 4096], P('ep', 'tp'), may hold values from -0.09375 to 0.09375
- w_down: bfloat16 [8, 1024, 4096], P('ep', 'tp'), may hold values from -0.1875 to 0.1875
- shared_hidden: bfloat16 [1024, 1024], P('ep'), may hold values from -4 to 4
Outputs:
- tokens_grad: bfloat16 [1024, 4096], P('ep', 'tp')
- gate_grad: float32 [1024, 2], P('ep')
- w_gate_grad: float32 [8, 1024, 4096], P('ep', 'tp')
- w_up_grad: float32 [8, 1024, 4096], P('ep', 'tp')
- w_down_grad: float32 [8, 1024, 4096], P('ep', 'tp')
- shared_grad: float32 [1024, 4096], P('ep', 'tp')
The draws below stay inside these ranges and needn't reach their ends.
Inputs may be any that keep to these rules, and one draw needn't show every extreme that they name: `routes`: each row names 2 different experts. Among the rows of one index of ep (aligned blocks of 128 rows) no expert is named more than 48 times, and in every draw some expert is named exactly 48 times in some block.
All inputs are finite; a program needn't handle non-finite values.
Results may differ from the reference program's by a relative error of at most 0.022.
Values may be sent and summed in bfloat16 or wider, within the bound.
A program may use at most 64 MiB of HBM per device.

```python
import math
import jax
import jax.numpy as jnp
import numpy as np
from jax import lax

D = 4096
HIDDEN_SIZE = 1024
SHARED_HIDDEN = 1024
TOP_K = 2
TOK_DEV = 128
EXPERTS = 8
CAP = 48
TOKENS = 1024
N_EP = 8
N_TP = 4


def with_spikes(drawn, rng, source, target, parts, factor):
    def block_of(position):
        return (jnp.arange(drawn.shape[position]) // (drawn.shape[position] // parts)).reshape((-1,) + (1,) * (drawn.ndim - 1 - position))

    near = jax.random.permutation(rng, parts)[block_of(target)]
    second = (block_of(target) + parts // 2) % parts
    return jnp.where((block_of(source) == near) | (block_of(source) == second), factor * drawn, drawn)


def levels(rng, shape, pieces, low, largest):
    def one(axis_at, shards_of):
        heights = jax.random.uniform(jax.random.fold_in(jax.random.fold_in(rng, 6), axis_at), (shards_of,), jnp.float32, low / len(pieces), largest / len(pieces))
        return jnp.repeat(jnp.exp(heights), shape[axis_at] // shards_of).reshape((-1,) + (1,) * (len(shape) - axis_at - 1))

    level = one(*pieces[0])
    for cut in pieces[1:]:
        level = level * one(*cut)
    return level


def deal_out(rng, own, number, rows, count, top, bound, lean):
    ranking = jax.random.permutation(rng, count)
    packed, common = portions_of(count, rows * top, bound, lean, True), portions_of(count, rows * top, bound, lean, False)
    places = jnp.arange(count)

    def named(tallies, turn):
        used = int((tallies > 0).sum())
        fixed = max(1, used // 4)
        moved = fixed + (places - fixed + turn * (used - fixed)) % max(1, count - fixed)
        return jnp.zeros((count,), jnp.int32).at[ranking[jnp.where(places < fixed, places, moved)]].set(jnp.asarray(tallies, jnp.int32))

    tallies = jnp.where(number % 4 == 0, named(packed, number // 4), named(common, number - number // 4 - 1))
    mixed = jax.random.permutation(jax.random.fold_in(own, 3), count)
    giver, receiver = mixed[0:count // 2 * 2:2], mixed[1:count // 2 * 2:2]
    room = jnp.minimum(tallies[giver] - 1, bound - tallies[receiver]) // 2
    room = jnp.where((giver == ranking[0]) | (receiver == ranking[0]) | (tallies[receiver] == 0), 0, jnp.maximum(room, 0))
    moved = jax.random.randint(jax.random.fold_in(own, 4), (count // 2,), 0, 1 << 20) % (room + 1)
    tallies = tallies.at[giver].add(-moved).at[receiver].add(moved)
    items = jnp.searchsorted(jnp.cumsum(tallies), jnp.arange(rows * top), side="right").astype(jnp.int32)
    table = items.reshape(top, rows).T
    table = table[jax.random.permutation(jax.random.fold_in(own, 1), rows)]
    turn = jax.random.randint(jax.random.fold_in(own, 2), (rows, 1), 0, top)
    return jnp.take_along_axis(table, (jnp.arange(top)[None, :] + turn) % top, axis=1)


def portions_of(count, total, limit, slope, full):
    portions = [(1 << 20) // math.isqrt(grade ** slope) + 1 for grade in range(1, count + 1)]
    largest = limit if full else min(limit, max(-(-total // count), total * portions[0] // sum(portions)))
    least = 1 if total - largest >= count - 1 else 0
    holding, surplus = [largest] + [least] * (count - 1), total - largest - least * (count - 1)
    while surplus > 0:
        movable = [i for i in range(1, count) if holding[i] < largest] or [i for i in range(1, count) if holding[i] < limit]
        whole, left = sum([portions[i] for i in movable]), surplus
        for i in movable:
            extra = min(limit - holding[i], max(1, left * portions[i] // whole), surplus)
            holding[i] = holding[i] + extra
            surplus = surplus - extra
    return np.array(holding)


def centred(key, dims, spread, bound, split=(), kind=jnp.bfloat16):
    drawn = spread * jax.random.normal(key, dims, jnp.float32)
    if split:
        drawn = drawn * levels(key, dims, split, -0.22, 0.18)
    return jnp.clip(drawn, -bound, bound).astype(kind)


def bell_draw_with(stream_key, extent, spread, most, cuts, heavy, kind=jnp.bfloat16):
    drawn = spread * jax.random.normal(stream_key, extent, jnp.float32)
    if cuts:
        drawn = drawn * levels(stream_key, extent, cuts, -0.22, 0.18)
    return jnp.clip(with_spikes(drawn, jax.random.fold_in(stream_key, 3), *heavy), -most, most).astype(kind)


def setup_inputs(seed: int = 0) -> dict:
    key_list = jax.random.split(jax.random.key(seed), 9)
    tokens = centred(key_list[0], (TOKENS, D), 1.0, 6.0, ((0, 8), (1, 4)))
    cotangent = centred(key_list[1], (TOKENS, D), 1.0, 6.0, ((0, 8), (1, 4)))
    routes_keys = jax.random.split(jax.random.fold_in(key_list[2], 1), TOKENS // TOK_DEV)
    routes_turns = jax.random.permutation(jax.random.fold_in(key_list[2], 3), TOKENS // TOK_DEV)
    routes = jax.vmap(lambda own, number: deal_out(jax.random.fold_in(key_list[2], 2), own, number, TOK_DEV, EXPERTS, TOP_K, CAP, 2))(routes_keys, routes_turns).reshape((TOKENS, TOP_K))
    gate_weight = jnp.clip(jnp.exp(math.log(2.5) - 3.218876 * jax.random.uniform(key_list[3], (TOKENS, TOP_K), jnp.float32) ** levels(key_list[3], (TOKENS, TOP_K), ((0, 8),), -0.2, 0.2)), 0.1, 2.5)
    w_gate = centred(key_list[4], (EXPERTS, HIDDEN_SIZE, D), D ** -0.5, 0.09375, ((0, 8), (1, 4)))
    w_up = centred(key_list[5], (EXPERTS, HIDDEN_SIZE, D), D ** -0.5, 0.09375, ((0, 8), (1, 4)))
    w_down = centred(key_list[6], (EXPERTS, HIDDEN_SIZE, D), HIDDEN_SIZE ** -0.5, 0.1875, ((0, 8), (1, 4)))
    shared_hidden = bell_draw_with(key_list[7], (TOKENS, SHARED_HIDDEN), 0.5, 4.0, ((0, 8),), (0, 1, 8, 2.0))
    return {"tokens": tokens, "cotangent": cotangent, "routes": routes, "gate_weight": gate_weight, "w_gate": w_gate, "w_up": w_up, "w_down": w_down, "shared_hidden": shared_hidden}


def slot_positions(device_routes):
    flat_routes = device_routes.reshape(-1)
    onehot = (flat_routes[:, None] == jnp.arange(EXPERTS, dtype=jnp.int32)[None, :]).astype(jnp.int32)
    earlier = jnp.cumsum(onehot, axis=0) - onehot
    return flat_routes, jnp.sum(earlier * onehot, axis=1).astype(jnp.int32)


def reference(tokens, cotangent, routes, gate_weight, w_gate, w_up, w_down, shared_hidden):
    assigned = TOK_DEV * TOP_K
    flat_routes, positions = jax.vmap(slot_positions)(routes.reshape(N_EP, assigned))
    sources = jnp.broadcast_to(jnp.arange(N_EP, dtype=jnp.int32)[:, None], (N_EP, assigned))
    token_ids = sources * TOK_DEV + jnp.arange(assigned, dtype=jnp.int32)[None, :] // TOP_K
    slot_table = jnp.full((EXPERTS, N_EP, CAP), TOKENS, jnp.int32).at[flat_routes, sources, positions].set(token_ids)
    weight_table = jnp.zeros((EXPERTS, N_EP, CAP), jnp.float32).at[flat_routes, sources, positions].set(
        gate_weight.reshape(N_EP, assigned))
    padded_tokens = jnp.concatenate([tokens, jnp.zeros((1, D), jnp.bfloat16)], 0)
    padded_cotan = jnp.concatenate([cotangent, jnp.zeros((1, D), jnp.bfloat16)], 0)
    groups = HIDDEN_SIZE // N_TP
    contract_last = (((1,), (1,)), ((), ()))

    def expert_fn(inputs):
        table_rows, weight_rows, gate_mat, up_mat, down_mat = inputs
        rows_x = padded_tokens[table_rows.reshape(-1)]
        rows_g = padded_cotan[table_rows.reshape(-1)]
        weight_col = weight_rows.reshape(-1, 1)
        pre_gate = lax.dot_general(rows_x, gate_mat, contract_last, preferred_element_type=jnp.float32)
        pre_up = lax.dot_general(rows_x, up_mat, contract_last, preferred_element_type=jnp.float32)
        sigmoid_gate = jax.nn.sigmoid(pre_gate)
        silu_gate = pre_gate * sigmoid_gate
        hidden = (silu_gate * pre_up).astype(jnp.bfloat16)
        back_hidden = lax.dot_general(rows_g, down_mat, contract_last, preferred_element_type=jnp.float32)
        gate_part = jnp.sum(hidden.astype(jnp.float32) * back_hidden, axis=1)
        scaled = weight_col * back_hidden
        grad_pre_gate = (scaled * pre_up * sigmoid_gate * (1.0 + pre_gate * (1.0 - sigmoid_gate))).astype(jnp.bfloat16)
        grad_pre_up = (scaled * silu_gate).astype(jnp.bfloat16)
        weighted_cotan = (weight_col * rows_g.astype(jnp.float32)).astype(jnp.bfloat16)
        grad_down = jnp.dot(hidden.T, weighted_cotan, preferred_element_type=jnp.float32)
        grad_gate = jnp.dot(grad_pre_gate.T, rows_x, preferred_element_type=jnp.float32)
        grad_up = jnp.dot(grad_pre_up.T, rows_x, preferred_element_type=jnp.float32)
        row_total = rows_x.shape[0]
        partial_value = jnp.einsum('rnh,nhd->nrd', grad_pre_gate.astype(jnp.float32).reshape(row_total, N_TP, groups),
                             gate_mat.astype(jnp.float32).reshape(N_TP, groups, D))
        partial_value = partial_value + jnp.einsum('rnh,nhd->nrd', grad_pre_up.astype(jnp.float32).reshape(row_total, N_TP, groups),
                                       up_mat.astype(jnp.float32).reshape(N_TP, groups, D))
        rounded = lax.optimization_barrier(partial_value.astype(jnp.bfloat16)).astype(jnp.float32)
        row_grad = jnp.sum(rounded, axis=0).astype(jnp.bfloat16)
        return row_grad.reshape(N_EP, CAP, D), gate_part.reshape(N_EP, CAP), grad_gate, grad_up, grad_down

    row_grads, gate_parts, w_gate_grad, w_up_grad, w_down_grad = lax.map(
        expert_fn, (slot_table, weight_table, w_gate, w_up, w_down))
    picked = row_grads[flat_routes, sources, positions].astype(jnp.float32)
    tokens_grad = jnp.sum(picked.reshape(TOKENS, TOP_K, D), axis=1).astype(jnp.bfloat16)
    gate_grad = gate_parts[flat_routes, sources, positions].reshape(TOKENS, TOP_K)
    shared_grad = jnp.dot(shared_hidden.T, cotangent, preferred_element_type=jnp.float32)
    return (tokens_grad, gate_grad, w_gate_grad, w_up_grad, w_down_grad, shared_grad)
```

```python
import functools

import jax
import jax.numpy as jnp
from jax import lax
from jax.experimental import pallas as pl
from jax.experimental.pallas import tpu as pltpu
from jax.sharding import PartitionSpec as P

MESH = pl.DeviceIdType.MESH
BF16 = jnp.bfloat16
F32 = jnp.float32
NT = (((1,), (1,)), ((), ()))
TN = (((0,), (0,)), ((), ()))


def routed_kernel(dims, *refs):
    E, T, X, C, F, N, K, H, hs = dims
    Y = T // 2
    NZ = E // X
    G = X * C
    tok_hbm, cot_hbm, routes_hbm, gates_hbm, sh_hbm, w_gate, w_up, w_down = refs[:8]
    xfull, gfull, hidden, grad_gate, grad_up, tokens_grad, gate_grad, shared_grad = refs[8:16]
    (
        wg,
        wu,
        wd,
        rows_out,
        meta_out,
        meta_in,
        cot_all,
        sh_in,
        gx_out,
        accs,
        part,
        pair_in,
        y_out,
        y_in,
        row_out,
        back,
        gate,
        gate_in,
        gate_out,
        gate_back,
        table,
        tg_acc,
        sg_acc,
        sg_out,
        sg_in,
        sh_t,
        tok,
        cot,
        routes,
        gates,
        sh,
    ) = refs[16:47]
    (
        load_sem,
        local_sem,
        meta_send,
        meta_recv,
        tok_send,
        tok_recv,
        sh_send,
        sh_recv,
        cot_up,
        cot_down,
        cot_recv,
        gx_send,
        gx_recv,
        y_send,
        y_recv,
        sib_send,
        sib_recv,
        pair_send,
        pair_recv,
        yr_send,
        yr_recv,
        back_send,
        back_recv,
        gate_tp_send,
        gate_tp_recv,
        gate_ep_send,
        gate_ep_recv,
        sg_send,
        sg_recv,
    ) = refs[47:]
    full = (xfull, gfull)
    me = lax.axis_index("ep")
    tp = lax.axis_index("tp")
    y = tp // 2
    c = tp % 2
    sib = y * 2 + (1 - c)
    z = me // X
    x = me % X

    barrier = pltpu.get_barrier_semaphore()

    def greet(d, _):
        pl.semaphore_signal(
            barrier, inc=1, device_id=((me + d) % E, tp), device_id_type=MESH
        )
        return 0

    lax.fori_loop(1, E, greet, 0)
    for dt in range(1, T):
        pl.semaphore_signal(
            barrier, inc=1, device_id=(me, (tp + dt) % T), device_id_type=MESH
        )

    loads = [
        pltpu.make_async_copy(src.at[0], dst, load_sem.at[i])
        for i, (src, dst) in enumerate(((w_gate, wg), (w_up, wu), (w_down, wd)))
    ]
    fetches = [
        pltpu.make_async_copy(src, dst, local_sem.at[i])
        for i, (src, dst) in enumerate(
            (
                (routes_hbm, routes),
                (gates_hbm, gates),
                (tok_hbm, tok),
                (cot_hbm, cot),
                (cot_hbm, cot_all.at[z]),
                (sh_hbm, sh),
            )
        )
    ]
    for cp in fetches:
        cp.start()
    for cp in loads:
        cp.start()
    for cp in fetches[:2]:
        cp.wait()

    def rows_of(s):
        return pl.ds(pl.multiple_of(s * C, 16), C)

    def group_of(zs):
        return pl.ds(pl.multiple_of(zs * G, 16), G)

    def cols_of(t):
        return pl.ds(pl.multiple_of(t * F, 128), F)

    def hidden_plane(zd):
        return pl.ds(pl.multiple_of(zd * X * hs, 16), X * hs)

    def remote(src, dst, ss, rs, dev):
        return pltpu.make_async_remote_copy(
            src_ref=src,
            dst_ref=dst,
            send_sem=ss,
            recv_sem=rs,
            device_id=dev,
            device_id_type=MESH,
        )

    def plane(j):
        near = jnp.minimum(z, NZ - 1 - z)
        swing = z + ((j + 1) // 2) * (1 - 2 * (j % 2))
        far = jnp.where(z < NZ - 1 - z, j, NZ - 1 - j)
        return jnp.where(j <= 2 * near, swing, far)

    expert = lax.broadcasted_iota(jnp.int32, (E, N), 0)
    hits = [routes[k : k + 1, :] == expert for k in range(K)]
    chosen = functools.reduce(jnp.logical_or, hits)
    weights = sum(jnp.where(h, gates[k : k + 1, :], 0.0) for k, h in enumerate(hits))
    earlier = (
        lax.broadcasted_iota(jnp.int32, (N, N), 0) < lax.broadcasted_iota(jnp.int32, (N, N), 1)
    ).astype(BF16)
    position = jnp.dot(chosen.astype(BF16), earlier, preferred_element_type=F32)
    position = jnp.where(chosen, position, -1.0)
    for e in range(E):
        meta_out[e // X, e % X : e % X + 1, :] = position[e : e + 1, :]
        meta_out[e // X, X + e % X : X + e % X + 1, :] = weights[e : e + 1, :]
    meta_in[me] = meta_out[z]
    for cp in fetches[2:4]:
        cp.wait()
    slot = lax.broadcasted_iota(jnp.int32, (C, N), 0).astype(F32)

    def pick(ref, s, row):
        return slot == ref[s, pl.ds(row, 1), :]

    def select(i, _):
        e = (me + i) % E
        chosen_rows = pick(meta_out, e // X, e % X).astype(BF16)
        table[rows_of(e), :] = chosen_rows
        rows_out[e] = jnp.dot(chosen_rows, tok[...], preferred_element_type=F32).astype(BF16)
        return 0

    lax.fori_loop(0, E, select, 0)
    xfull[rows_of(me), cols_of(tp)] = rows_out[me]
    gfull[rows_of(me), cols_of(tp)] = jnp.dot(
        table[rows_of(me), :], cot[...], preferred_element_type=F32
    ).astype(BF16)
    for cp in fetches[4:]:
        cp.wait()
    sh_t[...] = sh[...].T
    sh_in[z] = sh_t[hidden_plane(z), :]
    with jax.named_scope("barrier"):
        pl.semaphore_wait(barrier, (E - 1) + (T - 1))

    def meta_copy(dst):
        return remote(
            meta_out.at[dst // X], meta_in.at[me], meta_send.at[dst], meta_recv.at[me], (dst, tp)
        )

    def meta_wait(s):
        remote(
            meta_out.at[0], meta_in.at[s], meta_send.at[s], meta_recv.at[s], (me, tp)
        ).wait_recv()

    def tok_copy(dst):
        return remote(
            rows_out.at[dst],
            xfull.at[rows_of(me), cols_of(tp)],
            tok_send.at[dst],
            tok_recv.at[me],
            (dst, tp),
        )

    def sh_copy(zd):
        return remote(
            sh_t.at[hidden_plane(zd)],
            sh_in.at[z],
            sh_send.at[zd],
            sh_recv.at[z],
            (zd * X + x, tp),
        )

    def cot_copy(zs, sems, dst):
        return remote(cot_all.at[zs], cot_all.at[zs], sems.at[zs], cot_recv.at[zs], (dst, tp))

    def spread_cot(zs, act):
        @pl.when((zs <= z) & (z + 1 < NZ))
        def _():
            act(cot_copy(zs, cot_up, me + X))

        @pl.when((zs >= z) & (z >= 1))
        def _():
            act(cot_copy(zs, cot_down, me - X))

    def start(cp):
        cp.start()

    def wait_send(cp):
        cp.wait_send()

    def gx_copy(zs, d):
        return remote(
            gx_out.at[zs, d - 1],
            gfull.at[rows_of(zs * X + x), cols_of(tp)],
            gx_send.at[zs, d - 1],
            gx_recv.at[zs * X + x],
            (z * X + (x + d) % X, tp),
        )

    def y_copy(a, s, dy):
        piece = full[a].at[rows_of(s), cols_of(tp)]
        return remote(
            piece,
            piece,
            y_send.at[a, dy - 1],
            y_recv.at[a, dy - 1, s],
            (me, ((y + dy) % Y) * 2 + c),
        )

    def sib_copy(a, s, dy):
        piece = full[a].at[rows_of(s), cols_of(((y + Y - dy) % Y) * 2 + c)]
        return remote(
            piece, piece, sib_send.at[a, dy], sib_recv.at[a, dy, s // X], (me, sib)
        )

    def forward(a, s):
        for dy in range(1, Y):
            y_copy(a, s, dy).start()
        sib_copy(a, s, 0).start()

    def cross(zs):
        s = zs * X + x
        for d in range(1, X):
            xd = (x + d) % X
            gx_out[zs, d - 1] = jnp.dot(
                pick(meta_in, s, xd).astype(BF16), cot_all[zs], preferred_element_type=F32
            ).astype(BF16)
            gx_copy(zs, d).start()

    def others(fn):
        def step(j, _):
            zs = plane(j)
            for d in range(X):
                s = zs * X + (x + d) % X

                @pl.when(s != me)
                def _():
                    fn(s)

            return 0

        lax.fori_loop(0, NZ, step, 0)

    spread_cot(z, start)
    others(lambda s: meta_copy(s).start())
    cross(z)
    forward(1, me)
    others(lambda s: tok_copy(s).start())
    forward(0, me)

    def send_sh(j, _):
        sh_copy(plane(j)).start()
        return 0

    lax.fori_loop(1, NZ, send_sh, 0)

    def receive(j):
        zs = plane(j)
        s = zs * X + x

        @pl.when(j > 0)
        def _():
            remote(
                cot_all.at[zs], cot_all.at[zs], cot_up.at[zs], cot_recv.at[zs], (me, tp)
            ).wait_recv()
            spread_cot(zs, start)
            meta_wait(s)
            cross(zs)
            gfull[rows_of(s), cols_of(tp)] = jnp.dot(
                pick(meta_in, s, x).astype(BF16), cot_all[zs], preferred_element_type=F32
            ).astype(BF16)
            forward(1, s)

        for d in range(X):
            s = zs * X + (x + d) % X

            @pl.when(s != me)
            def _():
                remote(
                    rows_out.at[0],
                    xfull.at[rows_of(s), cols_of(tp)],
                    tok_send.at[s],
                    tok_recv.at[s],
                    (me, tp),
                ).wait_recv()
                forward(0, s)

        for d in range(1, X):
            s = zs * X + (x + d) % X
            remote(
                gx_out.at[0, 0],
                gfull.at[rows_of(s), cols_of(tp)],
                gx_send.at[0, 0],
                gx_recv.at[s],
                (me, tp),
            ).wait_recv()
            forward(1, s)

    def relay(j):
        zs = plane(j)
        for d in range(X):
            s = zs * X + (x + d) % X
            for a in (0, 1):
                for dy in range(1, Y):
                    piece = full[a].at[rows_of(s), cols_of(((y + Y - dy) % Y) * 2 + c)]
                    remote(
                        piece, piece, y_send.at[a, dy - 1], y_recv.at[a, dy - 1, s], (me, tp)
                    ).wait_recv()
                    sib_copy(a, s, dy).start()
            if d > 0:
                meta_wait(s)
        for a in (0, 1):
            for dy in range(Y):
                piece = full[a].at[group_of(zs), cols_of(((y + Y - dy) % Y) * 2 + 1 - c)]
                remote(
                    piece, piece, sib_send.at[a, dy], sib_recv.at[a, dy, zs], (me, sib)
                ).wait_recv()

    def pair_copy(zs, dy):
        return remote(
            part.at[group_of(zs), cols_of(((y + dy) % Y) * 2 + 1 - c)],
            pair_in.at[dy, group_of(zs)],
            pair_send.at[dy],
            pair_recv.at[dy, zs],
            (me, sib),
        )

    def compute(j):
        zs = plane(j)
        rows = group_of(zs)
        accs[...] = jnp.zeros_like(accs)

        @pl.when(j == 0)
        def _():
            for cp in loads:
                cp.wait()

        def ahead(t, _):
            cols = cols_of(t)
            for i, (v, w) in enumerate(((xfull, wg), (xfull, wu), (gfull, wd))):
                accs[i] += lax.dot_general(
                    v[rows, cols], w[:, cols], NT, preferred_element_type=F32
                )
            return 0

        lax.fori_loop(0, T, ahead, 0)
        for d in range(X):
            s = zs * X + d
            mine = slice(d * C, (d + 1) * C)
            picked = pick(meta_in, s, x)
            weight = jnp.sum(
                jnp.where(picked, meta_in[s, pl.ds(X + x, 1), :], 0.0), axis=1, keepdims=True
            )
            pre_gate = accs[0, mine, :]
            pre_up = accs[1, mine, :]
            behind = accs[2, mine, :]
            sigmoid_gate = jax.nn.sigmoid(pre_gate)
            silu_gate = pre_gate * sigmoid_gate
            hid = (silu_gate * pre_up).astype(BF16).astype(F32)
            column = jnp.sum(hid * behind, axis=1, keepdims=True)
            gate[pl.ds(s, 1), :] = jnp.sum(
                jnp.where(picked, column, 0.0), axis=0, keepdims=True
            )
            scaled = weight * behind
            hidden[rows_of(s), :] = (weight * hid).astype(BF16)
            grad_gate[rows_of(s), :] = (
                scaled * pre_up * sigmoid_gate * (1.0 + pre_gate * (1.0 - sigmoid_gate))
            ).astype(BF16)
            grad_up[rows_of(s), :] = (scaled * silu_gate).astype(BF16)

        def partial(t, _):
            cols = cols_of(t)
            part[rows, cols] = (
                jnp.dot(grad_gate[rows, :], wg[:, cols], preferred_element_type=F32)
                + jnp.dot(grad_up[rows, :], wu[:, cols], preferred_element_type=F32)
            ).astype(BF16)
            return 0

        lax.fori_loop(0, T, partial, 0)
        for dy in list(range(1, Y)) + [0]:
            pair_copy(zs, dy).start()

    def gate_tp_copy(dt):
        return remote(
            gate, gate_in.at[dt], gate_tp_send.at[dt], gate_tp_recv.at[dt], (me, (tp + dt) % T)
        )

    def share(j):
        zs = plane(j)

        @pl.when(j > 0)
        def _():
            remote(
                sh_t.at[hidden_plane(0)], sh_in.at[zs], sh_send.at[zs], sh_recv.at[zs], (me, tp)
            ).wait_recv()

        sg_acc[...] += jnp.dot(sh_in[zs], cot_all[zs], preferred_element_type=F32)

    def mix(zs, dy):
        rows = group_of(zs)
        pair_copy(zs, dy).wait_recv()
        return part[rows, cols_of(((y + dy) % Y) * 2 + c)].astype(F32) + pair_in[
            dy, rows, :
        ].astype(F32)

    def return_y(zs, dy):
        rows = group_of(zs)
        return remote(
            y_out.at[dy - 1, rows],
            y_in.at[dy - 1, rows],
            yr_send.at[dy - 1],
            yr_recv.at[dy - 1, zs],
            (me, ((y + dy) % Y) * 2 + c),
        )

    def combine(j):
        zs = plane(j)
        for dy in range(1, Y):
            y_out[dy - 1, group_of(zs), :] = mix(zs, dy).astype(BF16)
            return_y(zs, dy).start()

    def back_copy(s):
        return remote(
            row_out.at[rows_of(s)], back.at[rows_of(me)], back_send, back_recv.at[me], (s, tp)
        )

    def send_back(j):
        zs = plane(j)
        value = mix(zs, 0)
        for dy in range(1, Y):
            return_y(zs, dy).wait_recv()
            value = value + y_in[dy - 1, group_of(zs), :].astype(F32)
        row_out[group_of(zs), :] = value.astype(BF16)
        for d in range(X):
            s = zs * X + d

            @pl.when(s != me)
            def _():
                back_copy(s).start()

            @pl.when(s == me)
            def _():
                back[rows_of(s), :] = row_out[rows_of(s), :]

    sg_acc[...] = jnp.zeros_like(sg_acc)

    def main(i, _):
        @pl.when(i < NZ)
        def _():
            with jax.named_scope("receive"):
                receive(i)

        @pl.when((i >= 1) & (i <= NZ))
        def _():
            with jax.named_scope("relay"):
                relay(i - 1)
            with jax.named_scope("compute"):
                compute(i - 1)

        @pl.when(i == NZ)
        def _():
            for dt in range(1, T):
                gate_tp_copy(dt).start()

        @pl.when((i >= 1) & (i <= NZ))
        def _():
            with jax.named_scope("share"):
                share(i - 1)
            with jax.named_scope("combine"):
                combine(i - 1)

        @pl.when(i >= 2)
        def _():
            with jax.named_scope("send_back"):
                send_back(i - 2)

        return 0

    lax.fori_loop(0, NZ + 2, main, 0)

    def sg_copy(d):
        return remote(
            sg_out.at[d - 1],
            sg_in.at[d - 1],
            sg_send.at[d - 1],
            sg_recv.at[d - 1],
            (z * X + (x + d) % X, tp),
        )

    def hidden_of(xd):
        return pl.ds(pl.multiple_of(xd * hs, 16), hs)

    for d in range(1, X):
        sg_out[d - 1] = sg_acc[hidden_of((x + d) % X), :].astype(BF16)
        sg_copy(d).start()

    total = gate[...]
    for dt in range(1, T):
        gate_tp_copy(dt).wait()
        total = total + gate_in[dt]
    gate_out[...] = total
    gate_back[me] = total

    def gate_ep_copy(s):
        return remote(gate_out, gate_back.at[me], gate_ep_send, gate_ep_recv.at[me], (s, tp))

    others(lambda s: gate_ep_copy(s).start())

    value = sg_acc[hidden_of(x), :]
    for d in range(1, X):
        sg_copy(d).wait()
        value = value + sg_in[d - 1].astype(F32)
    shared_grad[...] = value

    tg_acc[...] = jnp.zeros_like(tg_acc)

    def gather(j, _):
        zs = plane(j)
        for d in range(X):
            e = zs * X + d

            @pl.when(e != me)
            def _():
                remote(
                    row_out.at[rows_of(e)],
                    back.at[rows_of(e)],
                    back_send,
                    back_recv.at[e],
                    (me, tp),
                ).wait_recv()

        tg_acc[...] += lax.dot_general(
            table[group_of(zs), :], back[group_of(zs), :], TN, preferred_element_type=F32
        )
        return 0

    with jax.named_scope("gather"):
        lax.fori_loop(0, NZ, gather, 0)
    tokens_grad[...] = tg_acc[...].astype(BF16)

    def take_gates(e, values):
        @pl.when(e != me)
        def _():
            remote(
                gate_out, gate_back.at[e], gate_ep_send, gate_ep_recv.at[e], (me, tp)
            ).wait_recv()

        row = gate_back[e, pl.ds(me, 1), :]
        return values + jnp.where(routes[...] == e, row, 0.0)

    gate_grad[...] = lax.fori_loop(0, E, take_gates, jnp.zeros((K, N), F32))

    def finish(s):
        meta_copy(s).wait_send()
        tok_copy(s).wait_send()
        gate_ep_copy(s).wait_send()
        back_copy(s).wait_send()

    others(finish)

    def finish_plane(j, _):
        zs = plane(j)

        @pl.when(j > 0)
        def _():
            sh_copy(zs).wait_send()

        spread_cot(zs, wait_send)
        for d in range(1, X):
            gx_copy(zs, d).wait_send()
        return 0

    lax.fori_loop(0, NZ, finish_plane, 0)
    for a in (0, 1):
        piece = full[a].at[:, cols_of(tp)]
        for dy in range(1, Y):
            remote(
                piece, piece, y_send.at[a, dy - 1], y_send.at[a, dy - 1], (me, sib)
            ).wait_send()
        for dy in range(Y):
            remote(
                piece, piece, sib_send.at[a, dy], sib_send.at[a, dy], (me, sib)
            ).wait_send()
    for dy in range(Y):
        piece = pair_in.at[dy]
        remote(piece, piece, pair_send.at[dy], pair_send.at[dy], (me, sib)).wait_send()
    for dy in range(1, Y):
        piece = y_in.at[dy - 1]
        remote(piece, piece, yr_send.at[dy - 1], yr_send.at[dy - 1], (me, sib)).wait_send()


def routed(E, T, C, F, N, hs, tokens, cotangent, routes, gates, shared, w_gate, w_up, w_down):
    X = 2 if E % 2 == 0 else 1
    NZ = E // X
    Y = T // 2
    Z = max(Y - 1, 1)
    XO = max(X - 1, 1)
    R = E * C
    H = w_gate.shape[1]
    K = routes.shape[0]
    M = -(-2 * X // 8) * 8
    dma = pltpu.SemaphoreType.DMA
    vmem = pl.BlockSpec(memory_space=pltpu.VMEM)
    hbm = pl.BlockSpec(memory_space=pltpu.HBM)
    shape = jax.ShapeDtypeStruct
    buffers = [
        pltpu.VMEM((H, T * F), BF16),
        pltpu.VMEM((H, T * F), BF16),
        pltpu.VMEM((H, T * F), BF16),
        pltpu.VMEM((E, C, F), BF16),
        pltpu.VMEM((NZ, M, N), F32),
        pltpu.VMEM((E, M, N), F32),
        pltpu.VMEM((NZ, N, F), BF16),
        pltpu.VMEM((NZ, X * hs, N), BF16),
        pltpu.VMEM((NZ, XO, C, F), BF16),
        pltpu.VMEM((3, X * C, H), F32),
        pltpu.VMEM((R, T * F), BF16),
        pltpu.VMEM((Y, R, F), BF16),
        pltpu.VMEM((Z, R, F), BF16),
        pltpu.VMEM((Z, R, F), BF16),
        pltpu.VMEM((R, F), BF16),
        pltpu.VMEM((R, F), BF16),
        pltpu.VMEM((E, N), F32),
        pltpu.VMEM((T, E, N), F32),
        pltpu.VMEM((E, N), F32),
        pltpu.VMEM((E, E, N), F32),
        pltpu.VMEM((R, N), BF16),
        pltpu.VMEM((N, F), F32),
        pltpu.VMEM((X * hs, F), F32),
        pltpu.VMEM((XO, hs, F), BF16),
        pltpu.VMEM((XO, hs, F), BF16),
        pltpu.VMEM((E * hs, N), BF16),
        pltpu.VMEM((N, F), BF16),
        pltpu.VMEM((N, F), BF16),
        pltpu.VMEM((K, N), jnp.int32),
        pltpu.VMEM((K, N), F32),
        pltpu.VMEM((N, E * hs), BF16),
    ]
    sems = [
        dma((3,)),
        dma((6,)),
        dma((E,)),
        dma((E,)),
        dma((E,)),
        dma((E,)),
        dma((NZ,)),
        dma((NZ,)),
        dma((NZ,)),
        dma((NZ,)),
        dma((NZ,)),
        dma((NZ, XO)),
        dma((E,)),
        dma((2, Z)),
        dma((2, Z, E)),
        dma((2, Y)),
        dma((2, Y, NZ)),
        dma((Y,)),
        dma((Y, NZ)),
        dma((Z,)),
        dma((Z, NZ)),
        dma,
        dma((E,)),
        dma((T,)),
        dma((T,)),
        dma,
        dma((E,)),
        dma((XO,)),
        dma((XO,)),
    ]
    return pl.pallas_call(
        functools.partial(routed_kernel, (E, T, X, C, F, N, K, H, hs)),
        out_shape=(
            shape((R, T * F), BF16),
            shape((R, T * F), BF16),
            shape((R, H), BF16),
            shape((R, H), BF16),
            shape((R, H), BF16),
            shape((N, F), BF16),
            shape((K, N), F32),
            shape((hs, F), F32),
        ),
        in_specs=[hbm] * 8,
        out_specs=(vmem,) * 8,
        scratch_shapes=buffers + sems,
        compiler_params=pltpu.CompilerParams(
            collective_id=0, has_side_effects=True, vmem_limit_bytes=36 * 1024 * 1024
        ),
        name="routed",
    )(
        *(
            pltpu.with_memory_space_constraint(v, pltpu.HBM)
            for v in (tokens, cotangent, routes, gates, shared, w_gate, w_up, w_down)
        )
    )


def weights_kernel(
    tile,
    rows_x,
    rows_g,
    hidden,
    grad_gate,
    grad_up,
    tokens_in,
    shared_in,
    gate_in,
    out_gate,
    out_up,
    out_down,
    tokens_out,
    shared_out,
    gate_out,
    buf,
    sem,
    small_sem,
):
    small = (
        pltpu.make_async_copy(tokens_in, tokens_out, small_sem.at[0]),
        pltpu.make_async_copy(shared_in, shared_out, small_sem.at[1]),
        pltpu.make_async_copy(gate_in, gate_out, small_sem.at[2]),
    )
    for cp in small:
        cp.start()
    plan = ((grad_gate, rows_x, out_gate), (grad_up, rows_x, out_up), (hidden, rows_g, out_down))
    steps = rows_x.shape[1] // tile

    def drain(i, slot, w):
        cols = pl.ds(pl.multiple_of(i * tile, 128), tile)
        return pltpu.make_async_copy(
            buf.at[slot, w], plan[w][2].at[0, :, cols], sem.at[slot, w]
        )

    def step(i, _):
        slot = i % 2
        cols = pl.ds(pl.multiple_of(i * tile, 128), tile)
        for w, (left, right, _) in enumerate(plan):

            @pl.when(i >= 2)
            def _():
                drain(i - 2, slot, w).wait()

            buf[slot, w] = lax.dot_general(
                left[...], right[:, cols], TN, preferred_element_type=F32
            )
            drain(i, slot, w).start()
        return 0

    lax.fori_loop(0, steps, step, 0)
    for i in range(max(steps - 2, 0), steps):
        for w in range(3):
            drain(i, i % 2, w).wait()
    for cp in small:
        cp.wait()


def weight_grads(
    rows_x, rows_g, hidden, grad_gate, grad_up, tokens_grad, shared_grad, gate_grad
):
    H = hidden.shape[1]
    D = rows_x.shape[1]
    tile = 512 if D % 512 == 0 else 128
    vmem = pl.BlockSpec(memory_space=pltpu.VMEM)
    hbm = pl.BlockSpec(memory_space=pltpu.HBM)
    shape = jax.ShapeDtypeStruct
    return pl.pallas_call(
        functools.partial(weights_kernel, tile),
        out_shape=(
            shape((1, H, D), F32),
            shape((1, H, D), F32),
            shape((1, H, D), F32),
            shape(tokens_grad.shape, BF16),
            shape(shared_grad.shape, F32),
            shape(gate_grad.shape, F32),
        ),
        in_specs=[vmem] * 8,
        out_specs=(hbm,) * 6,
        scratch_shapes=[
            pltpu.VMEM((2, 3, H, tile), F32),
            pltpu.SemaphoreType.DMA((2, 3)),
            pltpu.SemaphoreType.DMA((3,)),
        ],
        compiler_params=pltpu.CompilerParams(vmem_limit_bytes=16 * 1024 * 1024),
        name="weight_grads",
    )(rows_x, rows_g, hidden, grad_gate, grad_up, tokens_grad, shared_grad, gate_grad)


def shards(tokens, cotangent, routes, gate_weight, w_gate, w_up, w_down, shared_hidden):
    tok_count, top_count = routes.shape
    E = lax.axis_size("ep")
    T = lax.axis_size("tp")
    F = tokens.shape[1]
    capacity = 3 * tok_count * top_count // (2 * E)
    C = -(-capacity // 16) * 16
    hs = shared_hidden.shape[1] // E
    rows_x, rows_g, hidden, grad_gate, grad_up, tokens_grad, gate_grad, shared_grad = routed(
        E,
        T,
        C,
        F,
        tok_count,
        hs,
        tokens,
        cotangent,
        routes.T,
        gate_weight.T,
        shared_hidden,
        w_gate,
        w_up,
        w_down,
    )
    out_gate, out_up, out_down, tokens_grad, shared_grad, gate_grad = weight_grads(
        rows_x, rows_g, hidden, grad_gate, grad_up, tokens_grad, shared_grad, gate_grad
    )
    return (tokens_grad, gate_grad.T, out_gate, out_up, out_down, shared_grad)


def solution(mesh):
    placed = (
        P("ep", "tp"),
        P("ep", "tp"),
        P("ep", None),
        P("ep", None),
        P("ep", "tp", None),
        P("ep", "tp", None),
        P("ep", "tp", None),
        P("ep", None),
    )
    return jax.shard_map(
        shards,
        mesh=mesh,
        in_specs=placed,
        out_specs=(
            P("ep", "tp"),
            P("ep", None),
            P("ep", "tp", None),
            P("ep", "tp", None),
            P("ep", "tp", None),
            P("ep", "tp"),
        ),
        check_vma=False,
    )
```

```python
import functools

import jax
import jax.numpy as jnp
from jax import lax
from jax.experimental import pallas as pl
from jax.experimental.pallas import tpu as pltpu
from jax.sharding import PartitionSpec as P

MESH = pl.DeviceIdType.MESH
BF16 = jnp.bfloat16
F32 = jnp.float32
NT = (((1,), (1,)), ((), ()))
TN = (((0,), (0,)), ((), ()))


def routed_kernel(dims, *refs):
    E, T, X, C, F, N, K, H, hs = dims
    Y = T // 2
    NZ = E // X
    G = X * C
    tok_hbm, cot_hbm, routes_hbm, gates_hbm, sh_hbm, w_gate, w_up, w_down = refs[:8]
    out_gate, out_up, out_down, tokens_grad, gate_grad, shared_grad = refs[8:14]
    (
        wg,
        wu,
        wd,
        rows_out,
        meta_out,
        meta_in,
        cot_all,
        sh_in,
        gx_out,
        accs,
        part,
        pair_in,
        y_out,
        y_in,
        row_out,
        back,
        gate,
        gate_in,
        gate_out,
        gate_back,
        table,
        tg_acc,
        sg_acc,
        sg_out,
        sg_in,
        sh_t,
        tok,
        cot,
        routes,
        gates,
        sh,
        hid,
        gg,
        gu,
        turned,
        xfull,
        gfull,
        sides,
    ) = refs[14:52]
    (
        load_sem,
        local_sem,
        meta_send,
        meta_recv,
        tok_send,
        tok_recv,
        sh_send,
        sh_recv,
        cot_up,
        cot_down,
        cot_recv,
        gx_send,
        gx_recv,
        y_send,
        y_recv,
        sib_send,
        sib_recv,
        pair_send,
        pair_recv,
        yr_send,
        yr_recv,
        back_send,
        back_recv,
        gate_tp_send,
        gate_tp_recv,
        gate_ep_send,
        gate_ep_recv,
        sg_send,
        sg_recv,
        half_send,
        half_recv,
    ) = refs[52:]
    full = (xfull, gfull)
    me = lax.axis_index("ep")
    tp = lax.axis_index("tp")
    y = tp // 2
    c = tp % 2
    sib = y * 2 + (1 - c)
    z = me // X
    x = me % X

    barrier = pltpu.get_barrier_semaphore()

    def greet(d, _):
        pl.semaphore_signal(
            barrier, inc=1, device_id=((me + d) % E, tp), device_id_type=MESH
        )
        return 0

    lax.fori_loop(1, E, greet, 0)
    for dt in range(1, T):
        pl.semaphore_signal(
            barrier, inc=1, device_id=(me, (tp + dt) % T), device_id_type=MESH
        )

    loads = [
        pltpu.make_async_copy(src.at[0], dst, load_sem.at[i])
        for i, (src, dst) in enumerate(((w_gate, wg), (w_up, wu), (w_down, wd)))
    ]
    fetches = [
        pltpu.make_async_copy(src, dst, local_sem.at[i])
        for i, (src, dst) in enumerate(
            (
                (routes_hbm, routes),
                (gates_hbm, gates),
                (tok_hbm, tok),
                (cot_hbm, cot),
                (cot_hbm, cot_all.at[z]),
                (sh_hbm, sh),
            )
        )
    ]
    for cp in fetches:
        cp.start()
    for cp in fetches[:2]:
        cp.wait()

    def rows_of(s):
        return pl.ds(pl.multiple_of(s * C, 16), C)

    def group_of(zs):
        return pl.ds(pl.multiple_of(zs * G, 16), G)

    def cols_of(t):
        return pl.ds(pl.multiple_of(t * F, 128), F)

    def hidden_plane(zd):
        return pl.ds(pl.multiple_of(zd * X * hs, 16), X * hs)

    half = X * hs // 2

    def half_of(core):
        return pl.ds(pl.multiple_of(core * half, 16), half)

    def remote(src, dst, ss, rs, dev):
        return pltpu.make_async_remote_copy(
            src_ref=src,
            dst_ref=dst,
            send_sem=ss,
            recv_sem=rs,
            device_id=dev,
            device_id_type=MESH,
        )

    near = jnp.minimum(z, NZ - 1 - z)

    def plane(j):
        swing = z + ((j + 1) // 2) * (1 - 2 * (j % 2))
        far = jnp.where(z < NZ - 1 - z, j, NZ - 1 - j)
        return jnp.where(j <= 2 * near, swing, far)

    expert = lax.broadcasted_iota(jnp.int32, (E, N), 0)
    hits = [routes[k : k + 1, :] == expert for k in range(K)]
    chosen = functools.reduce(jnp.logical_or, hits)
    weights = sum(jnp.where(h, gates[k : k + 1, :], 0.0) for k, h in enumerate(hits))
    earlier = (
        lax.broadcasted_iota(jnp.int32, (N, N), 0) < lax.broadcasted_iota(jnp.int32, (N, N), 1)
    ).astype(BF16)
    position = jnp.dot(chosen.astype(BF16), earlier, preferred_element_type=F32)
    position = jnp.where(chosen, position, -1.0)
    for e in range(E):
        meta_out[e // X, e % X : e % X + 1, :] = position[e : e + 1, :]
        meta_out[e // X, X + e % X : X + e % X + 1, :] = weights[e : e + 1, :]
    meta_in[me] = meta_out[z]
    for cp in fetches[2:4]:
        cp.wait()
    slot = lax.broadcasted_iota(jnp.int32, (C, N), 0).astype(F32)

    def pick(ref, s, row):
        return slot == ref[s, pl.ds(row, 1), :]

    def select(e):
        chosen_rows = pick(meta_out, e // X, e % X).astype(BF16)
        table[rows_of(e), :] = chosen_rows
        rows_out[e] = jnp.dot(chosen_rows, tok[...], preferred_element_type=F32).astype(BF16)

    gfull[rows_of(me), cols_of(tp)] = jnp.dot(
        pick(meta_out, z, x).astype(BF16), cot[...], preferred_element_type=F32
    ).astype(BF16)
    for cp in fetches[4:]:
        cp.wait()
    with jax.named_scope("barrier"):
        pl.semaphore_wait(barrier, (E - 1) + (T - 1))

    def meta_copy(dst):
        return remote(
            meta_out.at[dst // X], meta_in.at[me], meta_send.at[dst], meta_recv.at[me], (dst, tp)
        )

    def meta_wait(s):
        remote(
            meta_out.at[0], meta_in.at[s], meta_send.at[s], meta_recv.at[s], (me, tp)
        ).wait_recv()

    def tok_copy(dst):
        return remote(
            rows_out.at[dst],
            xfull.at[rows_of(me), cols_of(tp)],
            tok_send.at[dst],
            tok_recv.at[me],
            (dst, tp),
        )

    def sh_copy(zd):
        return remote(
            sh_t.at[pl.ds(pl.multiple_of(zd * X * hs + c * half, 16), half)],
            sh_in.at[z, half_of(c)],
            sh_send.at[zd],
            sh_recv.at[z],
            (zd * X + x, tp),
        )

    def cot_copy(zs, sems, dst):
        return remote(cot_all.at[zs], cot_all.at[zs], sems.at[zs], cot_recv.at[zs], (dst, tp))

    def spread_cot(zs, act):
        @pl.when((zs <= z) & (z + 1 < NZ))
        def _():
            act(cot_copy(zs, cot_up, me + X))

        @pl.when((zs >= z) & (z >= 1))
        def _():
            act(cot_copy(zs, cot_down, me - X))

    def start(cp):
        cp.start()

    def wait_send(cp):
        cp.wait_send()

    def gx_copy(zs, d):
        return remote(
            gx_out.at[zs, d - 1],
            gfull.at[rows_of(zs * X + x), cols_of(tp)],
            gx_send.at[zs, d - 1],
            gx_recv.at[zs * X + x],
            (z * X + (x + d) % X, tp),
        )

    def y_copy(a, s, dy):
        piece = full[a].at[rows_of(s), cols_of(tp)]
        return remote(
            piece,
            piece,
            y_send.at[a, dy - 1],
            y_recv.at[a, dy - 1, s],
            (me, ((y + dy) % Y) * 2 + c),
        )

    def sib_copy(a, s, dy):
        piece = full[a].at[rows_of(s), cols_of(((y + Y - dy) % Y) * 2 + c)]
        return remote(
            piece, piece, sib_send.at[a, dy], sib_recv.at[a, dy, s // X], (me, sib)
        )

    def forward(a, s):
        for dy in range(1, Y):
            y_copy(a, s, dy).start()
        sib_copy(a, s, 0).start()

    def cross(zs):
        s = zs * X + x
        for d in range(1, X):
            xd = (x + d) % X
            gx_out[zs, d - 1] = jnp.dot(
                pick(meta_in, s, xd).astype(BF16), cot_all[zs], preferred_element_type=F32
            ).astype(BF16)
            gx_copy(zs, d).start()

    def others(fn):
        def step(j, _):
            zs = plane(j)
            for d in range(X):
                s = zs * X + (x + d) % X

                @pl.when(s != me)
                def _():
                    fn(s)

            return 0

        lax.fori_loop(0, NZ, step, 0)

    spread_cot(z, start)
    forward(1, me)
    others(lambda s: meta_copy(s).start())
    for cp in loads:
        cp.start()

    def send_rows(j):
        zs = plane(j)
        for d in range(X):
            s = zs * X + (x + d) % X
            select(s)

            @pl.when(s != me)
            def _():
                tok_copy(s).start()

    for d in range(1, X):
        select(z * X + (x + d) % X)
        tok_copy(z * X + (x + d) % X).start()
    send_rows(1)
    select(me)
    xfull[rows_of(me), cols_of(tp)] = rows_out[me]
    forward(0, me)
    cross(z)

    @pl.when(near >= 1)
    def _():
        send_rows(2)

    def send_late(i):
        j = jnp.where(near >= 1, i + 2, i + 1)

        @pl.when(j < NZ)
        def _():
            send_rows(j)

    sh_t[...] = sh[...].T
    sh_in[z] = sh_t[hidden_plane(z), :]

    def take_block(j):
        zs = plane(j)
        remote(
            cot_all.at[zs], cot_all.at[zs], cot_up.at[zs], cot_recv.at[zs], (me, tp)
        ).wait_recv()
        spread_cot(zs, start)

    def use_block(j):
        zs = plane(j)
        s = zs * X + x
        meta_wait(s)
        cross(zs)
        gfull[rows_of(s), cols_of(tp)] = jnp.dot(
            pick(meta_in, s, x).astype(BF16), cot_all[zs], preferred_element_type=F32
        ).astype(BF16)
        forward(1, s)

    def tokens_in(j):
        zs = plane(j)
        for d in range(X):
            s = zs * X + (x + d) % X

            @pl.when(s != me)
            def _():
                remote(
                    rows_out.at[0],
                    xfull.at[rows_of(s), cols_of(tp)],
                    tok_send.at[s],
                    tok_recv.at[s],
                    (me, tp),
                ).wait_recv()
                forward(0, s)

    def crossed(j):
        zs = plane(j)
        for d in range(1, X):
            s = zs * X + (x + d) % X
            remote(
                gx_out.at[0, 0],
                gfull.at[rows_of(s), cols_of(tp)],
                gx_send.at[0, 0],
                gx_recv.at[s],
                (me, tp),
            ).wait_recv()
            forward(1, s)

    def arrivals(i):
        first = (near == 0) | (i == 1)
        second = (near >= 1) & (i + 1 < NZ)
        for fn in (take_block, use_block, None, tokens_in, crossed):
            if fn is None:
                send_late(i)
                continue
            with jax.named_scope(fn.__name__):

                @pl.when(first)
                def _():
                    fn(i)

                @pl.when(second)
                def _():
                    fn(i + 1)

    def send_shared(j, _):
        sh_copy(plane(j)).start()
        return 0

    def relay(j):
        zs = plane(j)
        for d in range(X):
            s = zs * X + (x + d) % X
            for a in (0, 1):
                for dy in range(1, Y):
                    piece = full[a].at[rows_of(s), cols_of(((y + Y - dy) % Y) * 2 + c)]
                    remote(
                        piece, piece, y_send.at[a, dy - 1], y_recv.at[a, dy - 1, s], (me, tp)
                    ).wait_recv()
                    sib_copy(a, s, dy).start()
            if d > 0:
                meta_wait(s)
        for a in (0, 1):
            for dy in range(Y):
                piece = full[a].at[group_of(zs), cols_of(((y + Y - dy) % Y) * 2 + 1 - c)]
                remote(
                    piece, piece, sib_send.at[a, dy], sib_recv.at[a, dy, zs], (me, sib)
                ).wait_recv()

    def pair_copy(zs, dy):
        return remote(
            part.at[group_of(zs), cols_of(((y + dy) % Y) * 2 + 1 - c)],
            pair_in.at[dy, group_of(zs)],
            pair_send.at[dy],
            pair_recv.at[dy, zs],
            (me, sib),
        )

    def compute(j):
        zs = plane(j)
        rows = group_of(zs)
        with jax.named_scope("ahead"):
            for i, v in enumerate((xfull, xfull, gfull)):
                accs[i] = jnp.dot(v[rows, :], turned[i], preferred_element_type=F32)
        for d in range(X):
            s = zs * X + d
            mine = slice(d * C, (d + 1) * C)
            picked = pick(meta_in, s, x)
            weight = jnp.sum(
                jnp.where(picked, meta_in[s, pl.ds(X + x, 1), :], 0.0), axis=1, keepdims=True
            )
            pre_gate = accs[0, mine, :]
            pre_up = accs[1, mine, :]
            behind = accs[2, mine, :]
            sigmoid_gate = jax.nn.sigmoid(pre_gate)
            silu_gate = pre_gate * sigmoid_gate
            act = (silu_gate * pre_up).astype(BF16).astype(F32)
            column = jnp.sum(act * behind, axis=1, keepdims=True)
            gate[pl.ds(s, 1), :] = jnp.sum(
                jnp.where(picked, column, 0.0), axis=0, keepdims=True
            )
            scaled = weight * behind
            hid[rows_of(s), :] = (weight * act).astype(BF16)
            gg[rows_of(s), :] = (
                scaled * pre_up * sigmoid_gate * (1.0 + pre_gate * (1.0 - sigmoid_gate))
            ).astype(BF16)
            gu[rows_of(s), :] = (scaled * silu_gate).astype(BF16)

    def spread_rows(j):
        zs = plane(j)
        rows = group_of(zs)

        def partial(i, _):
            cols = cols_of((i % Y) * 2 + jnp.where(i < Y, 1 - c, c))
            part[rows, cols] = (
                jnp.dot(gg[rows, :], wg[:, cols], preferred_element_type=F32)
                + jnp.dot(gu[rows, :], wu[:, cols], preferred_element_type=F32)
            ).astype(BF16)
            return 0

        with jax.named_scope("partial"):
            lax.fori_loop(0, Y, partial, 0)
        for dy in list(range(1, Y)) + [0]:
            pair_copy(zs, dy).start()
        lax.fori_loop(Y, T, partial, 0)

    def gate_tp_copy(dt):
        return remote(
            gate, gate_in.at[dt], gate_tp_send.at[dt], gate_tp_recv.at[dt], (me, (tp + dt) % T)
        )

    def half_copy(zs, core):
        piece = sh_in.at[zs, half_of(core)]
        return remote(piece, piece, half_send.at[zs], half_recv.at[zs], (me, sib))

    def half_relay(j, _):
        zs = plane(j)
        piece = sh_in.at[zs, half_of(c)]
        remote(piece, piece, sh_send.at[zs], sh_recv.at[zs], (me, tp)).wait_recv()
        half_copy(zs, c).start()
        return 0

    def share(j, _):
        zs = plane(j)

        @pl.when(j > 0)
        def _():
            half_copy(zs, 1 - c).wait_recv()

        sg_acc[...] += jnp.dot(sh_in[zs], cot_all[zs], preferred_element_type=F32)
        return 0

    def mix(zs, dy):
        rows = group_of(zs)
        pair_copy(zs, dy).wait_recv()
        return part[rows, cols_of(((y + dy) % Y) * 2 + c)].astype(F32) + pair_in[
            dy, rows, :
        ].astype(F32)

    def return_y(zs, dy):
        rows = group_of(zs)
        return remote(
            y_out.at[dy - 1, rows],
            y_in.at[dy - 1, rows],
            yr_send.at[dy - 1],
            yr_recv.at[dy - 1, zs],
            (me, ((y + dy) % Y) * 2 + c),
        )

    def combine(j):
        zs = plane(j)
        for dy in range(1, Y):
            y_out[dy - 1, group_of(zs), :] = mix(zs, dy).astype(BF16)
            return_y(zs, dy).start()

    def back_copy(s):
        return remote(
            row_out.at[rows_of(s)], back.at[rows_of(me)], back_send, back_recv.at[me], (s, tp)
        )

    def send_back(j):
        zs = plane(j)
        value = mix(zs, 0)
        for dy in range(1, Y):
            return_y(zs, dy).wait_recv()
            value = value + y_in[dy - 1, group_of(zs), :].astype(F32)
        row_out[group_of(zs), :] = value.astype(BF16)
        for d in range(X):
            s = zs * X + d

            @pl.when(s != me)
            def _():
                back_copy(s).start()

            @pl.when(s == me)
            def _():
                back[rows_of(s), :] = row_out[rows_of(s), :]

    sg_acc[...] = jnp.zeros_like(sg_acc)

    def sg_copy(d):
        return remote(
            sg_out.at[d - 1],
            sg_in.at[d - 1],
            sg_send.at[d - 1],
            sg_recv.at[d - 1],
            (z * X + (x + d) % X, tp),
        )

    def hidden_of(xd):
        return pl.ds(pl.multiple_of(xd * hs, 16), hs)

    def turn(k):
        inward = jnp.where(2 * z < NZ - 1, 2, 1)
        outward = 3 - inward
        middle = jnp.where(k == 0, inward, jnp.where(k == 1, outward, (k + 1) % NZ))
        return jnp.where(near >= 1, middle, k)

    D = T * F
    tile = 512 if D % 512 == 0 else 128

    def weights_up():
        for n, src in enumerate((gg, gu, hid)):
            sides[n * H : (n + 1) * H, :] = src[...].T

        def step(i, _):
            cols = pl.ds(pl.multiple_of(i * tile, 128), tile)
            both = jnp.dot(sides[: 2 * H, :], xfull[:, cols], preferred_element_type=F32)
            out_gate[:, cols] = both[:H]
            out_up[:, cols] = both[H:]
            return 0

        lax.fori_loop(0, D // tile, step, 0)

    def weights_down():
        def step(i, _):
            cols = pl.ds(pl.multiple_of(i * tile, 128), tile)
            out_down[:, cols] = jnp.dot(
                sides[2 * H :, :], gfull[:, cols], preferred_element_type=F32
            )
            return 0

        lax.fori_loop(0, D // tile, step, 0)

    def main(i, _):
        @pl.when(i == 0)
        def _():
            tokens_in(i)
            crossed(i)

        @pl.when(i == 1)
        def _():
            for n, (cp, src) in enumerate(zip(loads, (wg, wu, wd))):
                cp.wait()
                turned[n] = src[...].T

        @pl.when((i >= 1) & (i < NZ))
        def _():
            arrivals(i)

        @pl.when(i == NZ - 1)
        def _():
            lax.fori_loop(1, NZ, send_shared, 0)

        @pl.when(i == NZ)
        def _():
            with jax.named_scope("share"):
                lax.fori_loop(1, NZ, half_relay, 0)
                combine(turn(NZ - 2))
                lax.fori_loop(0, NZ, share, 0)
                for d in range(1, X):
                    sg_out[d - 1] = sg_acc[hidden_of((x + d) % X), :].astype(BF16)
                    sg_copy(d).start()

        @pl.when((i >= 1) & (i <= NZ))
        def _():
            with jax.named_scope("relay"):
                relay(turn(i - 1))
            with jax.named_scope("compute"):
                compute(turn(i - 1))

        @pl.when((i >= 1) & (i <= NZ))
        def _():
            with jax.named_scope("partial"):
                spread_rows(turn(i - 1))

        @pl.when(i == NZ)
        def _():
            for dt in range(1, T):
                gate_tp_copy(dt).start()

        @pl.when(i == NZ + 1)
        def _():
            with jax.named_scope("weights_up"):
                weights_up()

        @pl.when(i >= 2)
        def _():
            with jax.named_scope("send_back"):
                send_back(turn(i - 2))

        @pl.when((i >= 1) & (i <= NZ) & (i != NZ - 1))
        def _():
            with jax.named_scope("combine"):
                combine(turn(i - 1))

        return 0

    lax.fori_loop(0, NZ + 2, main, 0)

    total = gate[...]
    with jax.named_scope("gate_tp"):
        for dt in range(1, T):
            gate_tp_copy(dt).wait()
    for dt in range(1, T):
        total = total + gate_in[dt]
    gate_out[...] = total
    gate_back[me] = total

    def gate_ep_copy(s):
        return remote(gate_out, gate_back.at[me], gate_ep_send, gate_ep_recv.at[me], (s, tp))

    others(lambda s: gate_ep_copy(s).start())

    value = sg_acc[hidden_of(x), :]
    with jax.named_scope("shared_in"):
        for d in range(1, X):
            sg_copy(d).wait()
    for d in range(1, X):
        value = value + sg_in[d - 1].astype(F32)
    shared_grad[...] = value

    with jax.named_scope("weights_down"):
        weights_down()
    tg_acc[...] = jnp.zeros_like(tg_acc)

    def gather(j, _):
        zs = plane(j)
        with jax.named_scope("back"):
            for d in range(X):
                e = zs * X + d

                @pl.when(e != me)
                def _():
                    remote(
                        row_out.at[rows_of(e)],
                        back.at[rows_of(e)],
                        back_send,
                        back_recv.at[e],
                        (me, tp),
                    ).wait_recv()

        tg_acc[...] += lax.dot_general(
            table[group_of(zs), :], back[group_of(zs), :], TN, preferred_element_type=F32
        )
        return 0

    with jax.named_scope("gather"):
        lax.fori_loop(0, NZ, gather, 0)
    tokens_grad[...] = tg_acc[...].astype(BF16)

    def take_gates(e, values):
        @pl.when(e != me)
        def _():
            remote(
                gate_out, gate_back.at[e], gate_ep_send, gate_ep_recv.at[e], (me, tp)
            ).wait_recv()

        row = gate_back[e, pl.ds(me, 1), :]
        return values + jnp.where(routes[...] == e, row, 0.0)

    with jax.named_scope("gates"):
        gate_grad[...] = lax.fori_loop(
            0, E, take_gates, jnp.zeros((K, N), F32)
        )

    def finish(s):
        meta_copy(s).wait_send()
        tok_copy(s).wait_send()
        gate_ep_copy(s).wait_send()
        back_copy(s).wait_send()

    with jax.named_scope("finish"):
        others(finish)

    def finish_plane(j, _):
        zs = plane(j)

        @pl.when(j > 0)
        def _():
            sh_copy(zs).wait_send()
            half_copy(zs, c).wait_send()

        spread_cot(zs, wait_send)
        for d in range(1, X):
            gx_copy(zs, d).wait_send()
        return 0

    lax.fori_loop(0, NZ, finish_plane, 0)
    for a in (0, 1):
        piece = full[a].at[:, cols_of(tp)]
        for dy in range(1, Y):
            remote(
                piece, piece, y_send.at[a, dy - 1], y_send.at[a, dy - 1], (me, sib)
            ).wait_send()
        for dy in range(Y):
            remote(
                piece, piece, sib_send.at[a, dy], sib_send.at[a, dy], (me, sib)
            ).wait_send()
    for dy in range(Y):
        piece = pair_in.at[dy]
        remote(piece, piece, pair_send.at[dy], pair_send.at[dy], (me, sib)).wait_send()
    for dy in range(1, Y):
        piece = y_in.at[dy - 1]
        remote(piece, piece, yr_send.at[dy - 1], yr_send.at[dy - 1], (me, sib)).wait_send()


def routed(E, T, C, F, N, hs, tokens, cotangent, routes, gates, shared, w_gate, w_up, w_down):
    X = 2 if E % 2 == 0 else 1
    NZ = E // X
    Y = T // 2
    Z = max(Y - 1, 1)
    XO = max(X - 1, 1)
    R = E * C
    H = w_gate.shape[1]
    K = routes.shape[0]
    M = -(-2 * X // 8) * 8
    dma = pltpu.SemaphoreType.DMA
    vmem = pl.BlockSpec(memory_space=pltpu.VMEM)
    hbm = pl.BlockSpec(memory_space=pltpu.HBM)
    shape = jax.ShapeDtypeStruct
    buffers = [
        pltpu.VMEM((H, T * F), BF16),
        pltpu.VMEM((H, T * F), BF16),
        pltpu.VMEM((H, T * F), BF16),
        pltpu.VMEM((E, C, F), BF16),
        pltpu.VMEM((NZ, M, N), F32),
        pltpu.VMEM((E, M, N), F32),
        pltpu.VMEM((NZ, N, F), BF16),
        pltpu.VMEM((NZ, X * hs, N), BF16),
        pltpu.VMEM((NZ, XO, C, F), BF16),
        pltpu.VMEM((3, X * C, H), F32),
        pltpu.VMEM((R, T * F), BF16),
        pltpu.VMEM((Y, R, F), BF16),
        pltpu.VMEM((Z, R, F), BF16),
        pltpu.VMEM((Z, R, F), BF16),
        pltpu.VMEM((R, F), BF16),
        pltpu.VMEM((R, F), BF16),
        pltpu.VMEM((E, N), F32),
        pltpu.VMEM((T, E, N), F32),
        pltpu.VMEM((E, N), F32),
        pltpu.VMEM((E, E, N), F32),
        pltpu.VMEM((R, N), BF16),
        pltpu.VMEM((N, F), F32),
        pltpu.VMEM((X * hs, F), F32),
        pltpu.VMEM((XO, hs, F), BF16),
        pltpu.VMEM((XO, hs, F), BF16),
        pltpu.VMEM((E * hs, N), BF16),
        pltpu.VMEM((N, F), BF16),
        pltpu.VMEM((N, F), BF16),
        pltpu.VMEM((K, N), jnp.int32),
        pltpu.VMEM((K, N), F32),
        pltpu.VMEM((N, E * hs), BF16),
        pltpu.VMEM((R, H), BF16),
        pltpu.VMEM((R, H), BF16),
        pltpu.VMEM((R, H), BF16),
        pltpu.VMEM((3, T * F, H), BF16),
        pltpu.VMEM((R, T * F), BF16),
        pltpu.VMEM((R, T * F), BF16),
        pltpu.VMEM((3 * H, R), BF16),
    ]
    sems = [
        dma((3,)),
        dma((6,)),
        dma((E,)),
        dma((E,)),
        dma((E,)),
        dma((E,)),
        dma((NZ,)),
        dma((NZ,)),
        dma((NZ,)),
        dma((NZ,)),
        dma((NZ,)),
        dma((NZ, XO)),
        dma((E,)),
        dma((2, Z)),
        dma((2, Z, E)),
        dma((2, Y)),
        dma((2, Y, NZ)),
        dma((Y,)),
        dma((Y, NZ)),
        dma((Z,)),
        dma((Z, NZ)),
        dma,
        dma((E,)),
        dma((T,)),
        dma((T,)),
        dma,
        dma((E,)),
        dma((XO,)),
        dma((XO,)),
        dma((NZ,)),
        dma((NZ,)),
    ]
    return pl.pallas_call(
        functools.partial(routed_kernel, (E, T, X, C, F, N, K, H, hs)),
        out_shape=(
            shape((H, T * F), F32),
            shape((H, T * F), F32),
            shape((H, T * F), F32),
            shape((N, F), BF16),
            shape((K, N), F32),
            shape((hs, F), F32),
        ),
        in_specs=[hbm] * 8,
        out_specs=(vmem,) * 6,
        scratch_shapes=buffers + sems,
        compiler_params=pltpu.CompilerParams(
            collective_id=0, has_side_effects=True, vmem_limit_bytes=40 * 1024 * 1024
        ),
        name="routed",
    )(
        *(
            pltpu.with_memory_space_constraint(v, pltpu.HBM)
            for v in (tokens, cotangent, routes, gates, shared, w_gate, w_up, w_down)
        )
    )


def store_kernel(count, *refs):
    sems = refs[-1]
    copies = [
        pltpu.make_async_copy(refs[i], refs[count + i], sems.at[i]) for i in range(count)
    ]
    for cp in copies:
        cp.start()
    for cp in copies:
        cp.wait()


def store(*arrays):
    count = len(arrays)
    return pl.pallas_call(
        functools.partial(store_kernel, count),
        out_shape=tuple(jax.ShapeDtypeStruct(v.shape, v.dtype) for v in arrays),
        in_specs=[pl.BlockSpec(memory_space=pltpu.VMEM)] * count,
        out_specs=(pl.BlockSpec(memory_space=pltpu.HBM),) * count,
        scratch_shapes=[pltpu.SemaphoreType.DMA((count,))],
        compiler_params=pltpu.CompilerParams(vmem_limit_bytes=16 * 1024 * 1024),
        name="store",
    )(*arrays)


def shards(tokens, cotangent, routes, gate_weight, w_gate, w_up, w_down, shared_hidden):
    tok_count, top_count = routes.shape
    E = lax.axis_size("ep")
    T = lax.axis_size("tp")
    F = tokens.shape[1]
    capacity = 3 * tok_count * top_count // (2 * E)
    C = -(-capacity // 16) * 16
    hs = shared_hidden.shape[1] // E
    results = routed(
        E,
        T,
        C,
        F,
        tok_count,
        hs,
        tokens,
        cotangent,
        routes.T,
        gate_weight.T,
        shared_hidden,
        w_gate,
        w_up,
        w_down,
    )
    out_gate, out_up, out_down, tokens_grad, gate_grad, shared_grad = store(*results)
    return (
        tokens_grad,
        gate_grad.T,
        out_gate[None],
        out_up[None],
        out_down[None],
        shared_grad,
    )


def solution(mesh):
    placed = (
        P("ep", "tp"),
        P("ep", "tp"),
        P("ep", None),
        P("ep", None),
        P("ep", "tp", None),
        P("ep", "tp", None),
        P("ep", "tp", None),
        P("ep", None),
    )
    return jax.shard_map(
        shards,
        mesh=mesh,
        in_specs=placed,
        out_specs=(
            P("ep", "tp"),
            P("ep", None),
            P("ep", "tp", None),
            P("ep", "tp", None),
            P("ep", "tp", None),
            P("ep", "tp"),
        ),
        check_vma=False,
    )
```

```python
import functools

import jax
import jax.numpy as jnp
from jax import lax
from jax.experimental import pallas as pl
from jax.experimental.pallas import tpu as pltpu
from jax.sharding import PartitionSpec as P

MESH = pl.DeviceIdType.MESH
BF16 = jnp.bfloat16
F32 = jnp.float32
NT = (((1,), (1,)), ((), ()))
TN = (((0,), (0,)), ((), ()))


def routed_kernel(dims, *refs):
    E, T, X, C, F, N, K, H, hs = dims
    Y = T // 2
    NZ = E // X
    G = X * C
    tok_hbm, cot_hbm, routes_hbm, gates_hbm, sh_hbm, w_gate, w_up, w_down = refs[:8]
    out_gate, out_up, out_down, tokens_grad, gate_grad, shared_grad = refs[8:14]
    (
        wg,
        wu,
        wd,
        rows_out,
        meta_out,
        meta_in,
        cot_all,
        sh_in,
        gx_out,
        accs,
        part,
        pair_in,
        y_out,
        y_in,
        row_out,
        back,
        gate,
        gate_in,
        gate_out,
        gate_back,
        table,
        tg_acc,
        sg_acc,
        sg_out,
        sg_in,
        sh_t,
        tok,
        cot,
        routes,
        gates,
        sh,
        hid,
        gg,
        gu,
        turned,
        xfull,
        gfull,
        sides,
    ) = refs[14:52]
    (
        load_sem,
        local_sem,
        meta_send,
        meta_recv,
        tok_send,
        tok_recv,
        sh_send,
        sh_recv,
        cot_up,
        cot_down,
        cot_recv,
        gx_send,
        gx_recv,
        y_send,
        y_recv,
        sib_send,
        sib_recv,
        pair_send,
        pair_recv,
        yr_send,
        yr_recv,
        back_send,
        back_recv,
        gate_tp_send,
        gate_tp_recv,
        gate_ep_send,
        gate_ep_recv,
        sg_send,
        sg_recv,
        half_send,
        half_recv,
    ) = refs[52:]
    full = (xfull, gfull)
    me = lax.axis_index("ep")
    tp = lax.axis_index("tp")
    y = tp // 2
    c = tp % 2
    sib = y * 2 + (1 - c)
    z = me // X
    x = me % X

    barrier = pltpu.get_barrier_semaphore()

    def greet(d, _):
        pl.semaphore_signal(
            barrier, inc=1, device_id=((me + d) % E, tp), device_id_type=MESH
        )
        return 0

    lax.fori_loop(1, E, greet, 0)
    for dt in range(1, T):
        pl.semaphore_signal(
            barrier, inc=1, device_id=(me, (tp + dt) % T), device_id_type=MESH
        )

    loads = [
        pltpu.make_async_copy(src.at[0], dst, load_sem.at[i])
        for i, (src, dst) in enumerate(((w_gate, wg), (w_up, wu), (w_down, wd)))
    ]
    fetches = [
        pltpu.make_async_copy(src, dst, local_sem.at[i])
        for i, (src, dst) in enumerate(
            (
                (routes_hbm, routes),
                (gates_hbm, gates),
                (tok_hbm, tok),
                (cot_hbm, cot),
                (cot_hbm, cot_all.at[z]),
                (sh_hbm, sh),
            )
        )
    ]
    for cp in fetches:
        cp.start()
    for cp in fetches[:2]:
        cp.wait()

    def rows_of(s):
        return pl.ds(pl.multiple_of(s * C, 16), C)

    def group_of(zs):
        return pl.ds(pl.multiple_of(zs * G, 16), G)

    def cols_of(t):
        return pl.ds(pl.multiple_of(t * F, 128), F)

    def hidden_plane(zd):
        return pl.ds(pl.multiple_of(zd * X * hs, 16), X * hs)

    half = X * hs // 2

    def half_of(core):
        return pl.ds(pl.multiple_of(core * half, 16), half)

    def remote(src, dst, ss, rs, dev):
        return pltpu.make_async_remote_copy(
            src_ref=src,
            dst_ref=dst,
            send_sem=ss,
            recv_sem=rs,
            device_id=dev,
            device_id_type=MESH,
        )

    near = jnp.minimum(z, NZ - 1 - z)

    def plane(j):
        swing = z + ((j + 1) // 2) * (1 - 2 * (j % 2))
        far = jnp.where(z < NZ - 1 - z, j, NZ - 1 - j)
        return jnp.where(j <= 2 * near, swing, far)

    expert = lax.broadcasted_iota(jnp.int32, (E, N), 0)
    hits = [routes[k : k + 1, :] == expert for k in range(K)]
    chosen = functools.reduce(jnp.logical_or, hits)
    weights = sum(jnp.where(h, gates[k : k + 1, :], 0.0) for k, h in enumerate(hits))
    earlier = (
        lax.broadcasted_iota(jnp.int32, (N, N), 0) < lax.broadcasted_iota(jnp.int32, (N, N), 1)
    ).astype(BF16)
    position = jnp.dot(chosen.astype(BF16), earlier, preferred_element_type=F32)
    position = jnp.where(chosen, position, -1.0)
    for e in range(E):
        meta_out[e // X, e % X : e % X + 1, :] = position[e : e + 1, :]
        meta_out[e // X, X + e % X : X + e % X + 1, :] = weights[e : e + 1, :]
    meta_in[me] = meta_out[z]
    for cp in fetches[2:4]:
        cp.wait()
    slot = lax.broadcasted_iota(jnp.int32, (C, N), 0).astype(F32)

    def pick(ref, s, row):
        return slot == ref[s, pl.ds(row, 1), :]

    def select(e):
        chosen_rows = pick(meta_out, e // X, e % X).astype(BF16)
        table[rows_of(e), :] = chosen_rows
        rows_out[e] = jnp.dot(chosen_rows, tok[...], preferred_element_type=F32).astype(BF16)

    gfull[rows_of(me), cols_of(tp)] = jnp.dot(
        pick(meta_out, z, x).astype(BF16), cot[...], preferred_element_type=F32
    ).astype(BF16)
    for cp in fetches[4:]:
        cp.wait()
    with jax.named_scope("barrier"):
        pl.semaphore_wait(barrier, (E - 1) + (T - 1))

    def meta_copy(dst):
        return remote(
            meta_out.at[dst // X], meta_in.at[me], meta_send.at[dst], meta_recv.at[me], (dst, tp)
        )

    def meta_wait(s):
        remote(
            meta_out.at[0], meta_in.at[s], meta_send.at[s], meta_recv.at[s], (me, tp)
        ).wait_recv()

    def tok_copy(dst):
        return remote(
            rows_out.at[dst],
            xfull.at[rows_of(me), cols_of(tp)],
            tok_send.at[dst],
            tok_recv.at[me],
            (dst, tp),
        )

    def sh_copy(zd):
        return remote(
            sh_t.at[pl.ds(pl.multiple_of(zd * X * hs + c * half, 16), half)],
            sh_in.at[z, half_of(c)],
            sh_send.at[zd],
            sh_recv.at[z],
            (zd * X + x, tp),
        )

    def cot_copy(zs, sems, dst):
        return remote(cot_all.at[zs], cot_all.at[zs], sems.at[zs], cot_recv.at[zs], (dst, tp))

    def spread_cot(zs, act):
        @pl.when((zs <= z) & (z + 1 < NZ))
        def _():
            act(cot_copy(zs, cot_up, me + X))

        @pl.when((zs >= z) & (z >= 1))
        def _():
            act(cot_copy(zs, cot_down, me - X))

    def start(cp):
        cp.start()

    def wait_send(cp):
        cp.wait_send()

    def gx_copy(zs, d):
        return remote(
            gx_out.at[zs, d - 1],
            gfull.at[rows_of(zs * X + x), cols_of(tp)],
            gx_send.at[zs, d - 1],
            gx_recv.at[zs * X + x],
            (z * X + (x + d) % X, tp),
        )

    def y_copy(a, s, dy):
        piece = full[a].at[rows_of(s), cols_of(tp)]
        return remote(
            piece,
            piece,
            y_send.at[a, dy - 1],
            y_recv.at[a, dy - 1, s],
            (me, ((y + dy) % Y) * 2 + c),
        )

    def sib_copy(a, s, dy):
        piece = full[a].at[rows_of(s), cols_of(((y + Y - dy) % Y) * 2 + c)]
        return remote(
            piece, piece, sib_send.at[a, dy], sib_recv.at[a, dy, s // X], (me, sib)
        )

    def forward(a, s):
        for dy in range(1, Y):
            y_copy(a, s, dy).start()
        sib_copy(a, s, 0).start()

    def cross(zs):
        s = zs * X + x
        for d in range(1, X):
            xd = (x + d) % X
            gx_out[zs, d - 1] = jnp.dot(
                pick(meta_in, s, xd).astype(BF16), cot_all[zs], preferred_element_type=F32
            ).astype(BF16)
            gx_copy(zs, d).start()

    def others(fn):
        def step(j, _):
            zs = plane(j)
            for d in range(X):
                s = zs * X + (x + d) % X

                @pl.when(s != me)
                def _():
                    fn(s)

            return 0

        lax.fori_loop(0, NZ, step, 0)

    spread_cot(z, start)
    forward(1, me)
    others(lambda s: meta_copy(s).start())
    for cp in loads:
        cp.start()

    def send_rows(j):
        zs = plane(j)
        for d in range(X):
            s = zs * X + (x + d) % X
            select(s)

            @pl.when(s != me)
            def _():
                tok_copy(s).start()

    for d in range(1, X):
        select(z * X + (x + d) % X)
        tok_copy(z * X + (x + d) % X).start()
    send_rows(1)
    select(me)
    xfull[rows_of(me), cols_of(tp)] = rows_out[me]
    forward(0, me)
    cross(z)

    @pl.when(near >= 1)
    def _():
        send_rows(2)

    def send_late(i):
        j = jnp.where(near >= 1, i + 2, i + 1)

        @pl.when(j < NZ)
        def _():
            send_rows(j)

    sh_t[...] = sh[...].T
    sh_in[z] = sh_t[hidden_plane(z), :]

    def take_block(j):
        zs = plane(j)
        remote(
            cot_all.at[zs], cot_all.at[zs], cot_up.at[zs], cot_recv.at[zs], (me, tp)
        ).wait_recv()
        spread_cot(zs, start)

    def use_block(j):
        zs = plane(j)
        s = zs * X + x
        meta_wait(s)
        cross(zs)
        gfull[rows_of(s), cols_of(tp)] = jnp.dot(
            pick(meta_in, s, x).astype(BF16), cot_all[zs], preferred_element_type=F32
        ).astype(BF16)
        forward(1, s)

    def tokens_in(j):
        zs = plane(j)
        for d in range(X):
            s = zs * X + (x + d) % X

            @pl.when(s != me)
            def _():
                remote(
                    rows_out.at[0],
                    xfull.at[rows_of(s), cols_of(tp)],
                    tok_send.at[s],
                    tok_recv.at[s],
                    (me, tp),
                ).wait_recv()
                forward(0, s)

    def crossed(j):
        zs = plane(j)
        for d in range(1, X):
            s = zs * X + (x + d) % X
            remote(
                gx_out.at[0, 0],
                gfull.at[rows_of(s), cols_of(tp)],
                gx_send.at[0, 0],
                gx_recv.at[s],
                (me, tp),
            ).wait_recv()
            forward(1, s)

    edge = near == 0

    def at(cond, fn, j):
        @pl.when(cond & (j < NZ))
        def _():
            with jax.named_scope(fn.__name__):
                fn(j)

    def arrivals(i):
        inner = near >= 1
        pair = inner & (i == 1)
        ahead = edge & ((i == 1) | (i == NZ - 1))
        for fn in (take_block, use_block):
            at(edge | pair, fn, i)
            at(pair, fn, i + 1)
        at(edge | pair, send_late, i)
        at(ahead | pair, tokens_in, i)
        at(pair, tokens_in, i + 1)
        at(ahead | pair, crossed, i)
        at(inner, crossed, i + 1)
        at(inner, take_block, i + 2)
        at(inner, use_block, i + 2)
        at(inner & (i >= 2), send_late, i)
        at(inner, tokens_in, i + 2)

    def late_arrivals(i):
        behind = edge & (i >= 2) & (i < NZ - 1)
        at(behind, crossed, i)
        at(behind, tokens_in, i)

    def send_shared(j, _):
        sh_copy(plane(j)).start()
        return 0

    def relay(j):
        zs = plane(j)
        for d in range(X):
            s = zs * X + (x + d) % X
            for a in (0, 1):
                for dy in range(1, Y):
                    piece = full[a].at[rows_of(s), cols_of(((y + Y - dy) % Y) * 2 + c)]
                    remote(
                        piece, piece, y_send.at[a, dy - 1], y_recv.at[a, dy - 1, s], (me, tp)
                    ).wait_recv()
                    sib_copy(a, s, dy).start()
            if d > 0:
                meta_wait(s)

    def settle(j):
        zs = plane(j)
        for a in (0, 1):
            for dy in range(Y):
                piece = full[a].at[group_of(zs), cols_of(((y + Y - dy) % Y) * 2 + 1 - c)]
                remote(
                    piece, piece, sib_send.at[a, dy], sib_recv.at[a, dy, zs], (me, sib)
                ).wait_recv()

    def pair_copy(zs, dy):
        return remote(
            part.at[group_of(zs), cols_of(((y + dy) % Y) * 2 + 1 - c)],
            pair_in.at[dy, group_of(zs)],
            pair_send.at[dy],
            pair_recv.at[dy, zs],
            (me, sib),
        )

    def compute(j):
        zs = plane(j)
        rows = group_of(zs)
        with jax.named_scope("ahead"):
            for i, v in enumerate((xfull, xfull, gfull)):
                accs[i] = jnp.dot(v[rows, :], turned[i], preferred_element_type=F32)
        for d in range(X):
            s = zs * X + d
            mine = slice(d * C, (d + 1) * C)
            picked = pick(meta_in, s, x)
            weight = jnp.sum(
                jnp.where(picked, meta_in[s, pl.ds(X + x, 1), :], 0.0), axis=1, keepdims=True
            )
            pre_gate = accs[0, mine, :]
            pre_up = accs[1, mine, :]
            behind = accs[2, mine, :]
            sigmoid_gate = jax.nn.sigmoid(pre_gate)
            silu_gate = pre_gate * sigmoid_gate
            act = (silu_gate * pre_up).astype(BF16).astype(F32)
            column = jnp.sum(act * behind, axis=1, keepdims=True)
            gate[pl.ds(s, 1), :] = jnp.sum(
                jnp.where(picked, column, 0.0), axis=0, keepdims=True
            )
            scaled = weight * behind
            hid[rows_of(s), :] = (weight * act).astype(BF16)
            gg[rows_of(s), :] = (
                scaled * pre_up * sigmoid_gate * (1.0 + pre_gate * (1.0 - sigmoid_gate))
            ).astype(BF16)
            gu[rows_of(s), :] = (scaled * silu_gate).astype(BF16)

    def spread_rows(j):
        zs = plane(j)
        rows = group_of(zs)

        def partial(i, _):
            cols = cols_of((i % Y) * 2 + jnp.where(i < Y, 1 - c, c))
            part[rows, cols] = (
                jnp.dot(gg[rows, :], wg[:, cols], preferred_element_type=F32)
                + jnp.dot(gu[rows, :], wu[:, cols], preferred_element_type=F32)
            ).astype(BF16)
            return 0

        with jax.named_scope("partial"):
            lax.fori_loop(0, Y, partial, 0)
        for dy in list(range(1, Y)) + [0]:
            pair_copy(zs, dy).start()
        lax.fori_loop(Y, T, partial, 0)

    def gate_tp_copy(dt):
        return remote(
            gate, gate_in.at[dt], gate_tp_send.at[dt], gate_tp_recv.at[dt], (me, (tp + dt) % T)
        )

    def half_copy(zs, core):
        piece = sh_in.at[zs, half_of(core)]
        return remote(piece, piece, half_send.at[zs], half_recv.at[zs], (me, sib))

    def half_relay(j, _):
        zs = plane(j)
        piece = sh_in.at[zs, half_of(c)]
        remote(piece, piece, sh_send.at[zs], sh_recv.at[zs], (me, tp)).wait_recv()
        half_copy(zs, c).start()
        return 0

    def share(j, _):
        zs = plane(j)

        @pl.when(j > 0)
        def _():
            half_copy(zs, 1 - c).wait_recv()

        sg_acc[...] += jnp.dot(sh_in[zs], cot_all[zs], preferred_element_type=F32)
        return 0

    def mix(zs, dy):
        rows = group_of(zs)
        pair_copy(zs, dy).wait_recv()
        return part[rows, cols_of(((y + dy) % Y) * 2 + c)].astype(F32) + pair_in[
            dy, rows, :
        ].astype(F32)

    def return_y(zs, dy):
        rows = group_of(zs)
        return remote(
            y_out.at[dy - 1, rows],
            y_in.at[dy - 1, rows],
            yr_send.at[dy - 1],
            yr_recv.at[dy - 1, zs],
            (me, ((y + dy) % Y) * 2 + c),
        )

    def combine(j):
        zs = plane(j)
        for dy in range(1, Y):
            y_out[dy - 1, group_of(zs), :] = mix(zs, dy).astype(BF16)
            return_y(zs, dy).start()

    def back_copy(s):
        return remote(
            row_out.at[rows_of(s)], back.at[rows_of(me)], back_send, back_recv.at[me], (s, tp)
        )

    def send_back(j):
        zs = plane(j)
        value = mix(zs, 0)
        for dy in range(1, Y):
            return_y(zs, dy).wait_recv()
            value = value + y_in[dy - 1, group_of(zs), :].astype(F32)
        row_out[group_of(zs), :] = value.astype(BF16)
        for d in range(X):
            s = zs * X + d

            @pl.when(s != me)
            def _():
                back_copy(s).start()

            @pl.when(s == me)
            def _():
                back[rows_of(s), :] = row_out[rows_of(s), :]

    sg_acc[...] = jnp.zeros_like(sg_acc)

    def sg_copy(d):
        return remote(
            sg_out.at[d - 1],
            sg_in.at[d - 1],
            sg_send.at[d - 1],
            sg_recv.at[d - 1],
            (z * X + (x + d) % X, tp),
        )

    def hidden_of(xd):
        return pl.ds(pl.multiple_of(xd * hs, 16), hs)

    def turn(k):
        inward = jnp.where(2 * z < NZ - 1, 2, 1)
        outward = 3 - inward
        middle = jnp.where(k == 0, inward, jnp.where(k == 1, outward, (k + 1) % NZ))
        return jnp.where(near >= 1, middle, k)

    D = T * F
    tile = 512 if D % 512 == 0 else 128

    def weights_up():
        for n, src in enumerate((gg, gu, hid)):
            sides[n * H : (n + 1) * H, :] = src[...].T

        def step(i, _):
            cols = pl.ds(pl.multiple_of(i * tile, 128), tile)
            both = jnp.dot(sides[: 2 * H, :], xfull[:, cols], preferred_element_type=F32)
            out_gate[:, cols] = both[:H]
            out_up[:, cols] = both[H:]
            return 0

        lax.fori_loop(0, D // tile, step, 0)

    def weights_down():
        def step(i, _):
            cols = pl.ds(pl.multiple_of(i * tile, 128), tile)
            out_down[:, cols] = jnp.dot(
                sides[2 * H :, :], gfull[:, cols], preferred_element_type=F32
            )
            return 0

        lax.fori_loop(0, D // tile, step, 0)

    def main(i, _):
        @pl.when(i == 0)
        def _():
            tokens_in(i)
            crossed(i)

        @pl.when(i == 1)
        def _():
            for n, (cp, src) in enumerate(zip(loads, (wg, wu, wd))):
                cp.wait()
                turned[n] = src[...].T

        @pl.when((i >= 1) & (i < NZ))
        def _():
            arrivals(i)

        @pl.when(i == NZ - 1)
        def _():
            lax.fori_loop(1, NZ, send_shared, 0)

        @pl.when((i >= 1) & (i <= NZ))
        def _():
            with jax.named_scope("relay"):

                @pl.when((near == 0) | (i == 1))
                def _():
                    relay(turn(i - 1))

                settle(turn(i - 1))
            with jax.named_scope("compute"):
                compute(turn(i - 1))

        @pl.when((i >= 1) & (i <= NZ))
        def _():
            with jax.named_scope("partial"):
                spread_rows(turn(i - 1))

            @pl.when((near >= 1) & (i < NZ))
            def _():
                with jax.named_scope("next_relay"):
                    relay(turn(i))

        @pl.when(i == NZ)
        def _():
            for dt in range(1, T):
                gate_tp_copy(dt).start()
            lax.fori_loop(1, NZ, half_relay, 0)

        @pl.when(i == NZ + 1)
        def _():
            with jax.named_scope("share"):
                lax.fori_loop(0, NZ, share, 0)
                for d in range(1, X):
                    sg_out[d - 1] = sg_acc[hidden_of((x + d) % X), :].astype(BF16)
                    sg_copy(d).start()
            with jax.named_scope("weights_up"):
                weights_up()

        @pl.when(i >= 2)
        def _():
            with jax.named_scope("send_back"):
                send_back(turn(i - 2))

        @pl.when((i >= 1) & (i <= NZ))
        def _():
            with jax.named_scope("combine"):
                combine(turn(i - 1))

        late_arrivals(i)
        return 0

    lax.fori_loop(0, NZ + 2, main, 0)

    total = gate[...]
    with jax.named_scope("gate_tp"):
        for dt in range(1, T):
            gate_tp_copy(dt).wait()
    for dt in range(1, T):
        total = total + gate_in[dt]
    gate_out[...] = total
    gate_back[me] = total

    def gate_ep_copy(s):
        return remote(gate_out, gate_back.at[me], gate_ep_send, gate_ep_recv.at[me], (s, tp))

    others(lambda s: gate_ep_copy(s).start())

    with jax.named_scope("weights_down"):
        weights_down()
    tg_acc[...] = jnp.zeros_like(tg_acc)

    def gather(j, _):
        zs = plane(j)
        with jax.named_scope("back"):
            for d in range(X):
                e = zs * X + d

                @pl.when(e != me)
                def _():
                    remote(
                        row_out.at[rows_of(e)],
                        back.at[rows_of(e)],
                        back_send,
                        back_recv.at[e],
                        (me, tp),
                    ).wait_recv()

        tg_acc[...] += lax.dot_general(
            table[group_of(zs), :], back[group_of(zs), :], TN, preferred_element_type=F32
        )
        return 0

    with jax.named_scope("gather"):
        lax.fori_loop(0, NZ, gather, 0)
    tokens_grad[...] = tg_acc[...].astype(BF16)

    def take_gates(e, values):
        @pl.when(e != me)
        def _():
            remote(
                gate_out, gate_back.at[e], gate_ep_send, gate_ep_recv.at[e], (me, tp)
            ).wait_recv()

        row = gate_back[e, pl.ds(me, 1), :]
        return values + jnp.where(routes[...] == e, row, 0.0)

    with jax.named_scope("gates"):
        gate_grad[...] = lax.fori_loop(
            0, E, take_gates, jnp.zeros((K, N), F32)
        )

    value = sg_acc[hidden_of(x), :]
    with jax.named_scope("shared_in"):
        for d in range(1, X):
            sg_copy(d).wait()
    for d in range(1, X):
        value = value + sg_in[d - 1].astype(F32)
    shared_grad[...] = value

    def finish(s):
        meta_copy(s).wait_send()
        tok_copy(s).wait_send()
        gate_ep_copy(s).wait_send()
        back_copy(s).wait_send()

    with jax.named_scope("finish"):
        others(finish)

    def finish_plane(j, _):
        zs = plane(j)

        @pl.when(j > 0)
        def _():
            sh_copy(zs).wait_send()
            half_copy(zs, c).wait_send()

        spread_cot(zs, wait_send)
        for d in range(1, X):
            gx_copy(zs, d).wait_send()
        return 0

    lax.fori_loop(0, NZ, finish_plane, 0)
    for a in (0, 1):
        piece = full[a].at[:, cols_of(tp)]
        for dy in range(1, Y):
            remote(
                piece, piece, y_send.at[a, dy - 1], y_send.at[a, dy - 1], (me, sib)
            ).wait_send()
        for dy in range(Y):
            remote(
                piece, piece, sib_send.at[a, dy], sib_send.at[a, dy], (me, sib)
            ).wait_send()
    for dy in range(Y):
        piece = pair_in.at[dy]
        remote(piece, piece, pair_send.at[dy], pair_send.at[dy], (me, sib)).wait_send()
    for dy in range(1, Y):
        piece = y_in.at[dy - 1]
        remote(piece, piece, yr_send.at[dy - 1], yr_send.at[dy - 1], (me, sib)).wait_send()


def routed(E, T, C, F, N, hs, tokens, cotangent, routes, gates, shared, w_gate, w_up, w_down):
    X = 2 if E % 2 == 0 else 1
    NZ = E // X
    Y = T // 2
    Z = max(Y - 1, 1)
    XO = max(X - 1, 1)
    R = E * C
    H = w_gate.shape[1]
    K = routes.shape[0]
    M = -(-2 * X // 8) * 8
    dma = pltpu.SemaphoreType.DMA
    vmem = pl.BlockSpec(memory_space=pltpu.VMEM)
    hbm = pl.BlockSpec(memory_space=pltpu.HBM)
    shape = jax.ShapeDtypeStruct
    buffers = [
        pltpu.VMEM((H, T * F), BF16),
        pltpu.VMEM((H, T * F), BF16),
        pltpu.VMEM((H, T * F), BF16),
        pltpu.VMEM((E, C, F), BF16),
        pltpu.VMEM((NZ, M, N), F32),
        pltpu.VMEM((E, M, N), F32),
        pltpu.VMEM((NZ, N, F), BF16),
        pltpu.VMEM((NZ, X * hs, N), BF16),
        pltpu.VMEM((NZ, XO, C, F), BF16),
        pltpu.VMEM((3, X * C, H), F32),
        pltpu.VMEM((R, T * F), BF16),
        pltpu.VMEM((Y, R, F), BF16),
        pltpu.VMEM((Z, R, F), BF16),
        pltpu.VMEM((Z, R, F), BF16),
        pltpu.VMEM((R, F), BF16),
        pltpu.VMEM((R, F), BF16),
        pltpu.VMEM((E, N), F32),
        pltpu.VMEM((T, E, N), F32),
        pltpu.VMEM((E, N), F32),
        pltpu.VMEM((E, E, N), F32),
        pltpu.VMEM((R, N), BF16),
        pltpu.VMEM((N, F), F32),
        pltpu.VMEM((X * hs, F), F32),
        pltpu.VMEM((XO, hs, F), BF16),
        pltpu.VMEM((XO, hs, F), BF16),
        pltpu.VMEM((E * hs, N), BF16),
        pltpu.VMEM((N, F), BF16),
        pltpu.VMEM((N, F), BF16),
        pltpu.VMEM((K, N), jnp.int32),
        pltpu.VMEM((K, N), F32),
        pltpu.VMEM((N, E * hs), BF16),
        pltpu.VMEM((R, H), BF16),
        pltpu.VMEM((R, H), BF16),
        pltpu.VMEM((R, H), BF16),
        pltpu.VMEM((3, T * F, H), BF16),
        pltpu.VMEM((R, T * F), BF16),
        pltpu.VMEM((R, T * F), BF16),
        pltpu.VMEM((3 * H, R), BF16),
    ]
    sems = [
        dma((3,)),
        dma((6,)),
        dma((E,)),
        dma((E,)),
        dma((E,)),
        dma((E,)),
        dma((NZ,)),
        dma((NZ,)),
        dma((NZ,)),
        dma((NZ,)),
        dma((NZ,)),
        dma((NZ, XO)),
        dma((E,)),
        dma((2, Z)),
        dma((2, Z, E)),
        dma((2, Y)),
        dma((2, Y, NZ)),
        dma((Y,)),
        dma((Y, NZ)),
        dma((Z,)),
        dma((Z, NZ)),
        dma,
        dma((E,)),
        dma((T,)),
        dma((T,)),
        dma,
        dma((E,)),
        dma((XO,)),
        dma((XO,)),
        dma((NZ,)),
        dma((NZ,)),
    ]
    return pl.pallas_call(
        functools.partial(routed_kernel, (E, T, X, C, F, N, K, H, hs)),
        out_shape=(
            shape((H, T * F), F32),
            shape((H, T * F), F32),
            shape((H, T * F), F32),
            shape((N, F), BF16),
            shape((K, N), F32),
            shape((hs, F), F32),
        ),
        in_specs=[hbm] * 8,
        out_specs=(vmem,) * 6,
        scratch_shapes=buffers + sems,
        compiler_params=pltpu.CompilerParams(
            collective_id=0, has_side_effects=True, vmem_limit_bytes=40 * 1024 * 1024
        ),
        name="routed",
    )(
        *(
            pltpu.with_memory_space_constraint(v, pltpu.HBM)
            for v in (tokens, cotangent, routes, gates, shared, w_gate, w_up, w_down)
        )
    )


def store_kernel(count, *refs):
    sems = refs[-1]
    copies = [
        pltpu.make_async_copy(refs[i], refs[count + i], sems.at[i]) for i in range(count)
    ]
    for cp in copies:
        cp.start()
    for cp in copies:
        cp.wait()


def store(*arrays):
    count = len(arrays)
    return pl.pallas_call(
        functools.partial(store_kernel, count),
        out_shape=tuple(jax.ShapeDtypeStruct(v.shape, v.dtype) for v in arrays),
        in_specs=[pl.BlockSpec(memory_space=pltpu.VMEM)] * count,
        out_specs=(pl.BlockSpec(memory_space=pltpu.HBM),) * count,
        scratch_shapes=[pltpu.SemaphoreType.DMA((count,))],
        compiler_params=pltpu.CompilerParams(vmem_limit_bytes=16 * 1024 * 1024),
        name="store",
    )(*arrays)


def shards(tokens, cotangent, routes, gate_weight, w_gate, w_up, w_down, shared_hidden):
    tok_count, top_count = routes.shape
    E = lax.axis_size("ep")
    T = lax.axis_size("tp")
    F = tokens.shape[1]
    capacity = 3 * tok_count * top_count // (2 * E)
    C = -(-capacity // 16) * 16
    hs = shared_hidden.shape[1] // E
    results = routed(
        E,
        T,
        C,
        F,
        tok_count,
        hs,
        tokens,
        cotangent,
        routes.T,
        gate_weight.T,
        shared_hidden,
        w_gate,
        w_up,
        w_down,
    )
    out_gate, out_up, out_down, tokens_grad, gate_grad, shared_grad = store(*results)
    return (
        tokens_grad,
        gate_grad.T,
        out_gate[None],
        out_up[None],
        out_down[None],
        shared_grad,
    )


def solution(mesh):
    placed = (
        P("ep", "tp"),
        P("ep", "tp"),
        P("ep", None),
        P("ep", None),
        P("ep", "tp", None),
        P("ep", "tp", None),
        P("ep", "tp", None),
        P("ep", None),
    )
    return jax.shard_map(
        shards,
        mesh=mesh,
        in_specs=placed,
        out_specs=(
            P("ep", "tp"),
            P("ep", None),
            P("ep", "tp", None),
            P("ep", "tp", None),
            P("ep", "tp", None),
            P("ep", "tp"),
        ),
        check_vma=False,
    )
```
